128 devices in a mesh: sp: 16 (over z, y), tp: 8 (over x, core).
Axes of the slice: x: 4, y: 4, z: 4, core: 2. Of those that a mesh axis runs over, the one named last changes fastest.
Arguments:
- tokens: bfloat16 [32768, 2048], P('sp'), may hold values from -6 to 6
- w_query: bfloat16 [2048, 1024], P(None, 'tp'), may hold values from -0.125 to 0.125
- w_key: bfloat16 [2048, 1024], P(None, 'tp'), may hold values from -0.125 to 0.125
- w_value: bfloat16 [2048, 1024], P(None, 'tp'), may hold values from -0.125 to 0.125
- w_gate: bfloat16 [2048, 1024], P(None, 'tp'), may hold values from -0.125 to 0.125
- w_pool: bfloat16 [2048, 1024], P(None, 'tp'), may hold values from -0.125 to 0.125
- norm_gain: float32 [1024], P('tp'), may hold values from 0.1 to 1.9
- log_decay: float32 [8, 32768], P('tp', 'sp'), may hold values from -0.8 to 0
- w_out: bfloat16 [2048, 2048], replicated, may hold values from -0.125 to 0.125
Outputs:
- mixed_out: bfloat16 [32768, 2048], P(('sp', 'tp'))
The draws below stay inside these ranges and needn't reach their ends.
All inputs are finite; a program needn't handle non-finite values.
Results may differ from the reference program's by a relative error of at most 0.014.
Values may be sent and summed in bfloat16 or wider, within the bound.
A program may use at most 64 MiB of HBM per device.

```python
import jax
import jax.numpy as jnp
from jax import lax

D = 2048
RETENTION_HEADS = 8
HEAD_DIM = 128
POOL_GROUP = 256
BLOCK = 128
TOK_DEV = 2048
RET_WIDTH = 1024
POOL_WIDTH = 1024
SEQUENCE_TOKENS = 32768


def draw_log_decay(key, part):
    key_perm, key_fast, key_slow, key_dev, key_position, key_level = jax.random.split(jax.random.fold_in(key, 11), 6)
    order = jax.random.permutation(key_perm, RETENTION_HEADS)
    slow_heads = order < RETENTION_HEADS // 2
    fast_rate = jnp.exp(jax.random.uniform(key_fast, (RETENTION_HEADS,), jnp.float32, jnp.log(1.0 / 60.0), jnp.log(1.0 / 25.0)))
    slow_rate = jnp.exp(jax.random.uniform(key_slow, (RETENTION_HEADS,), jnp.float32, jnp.log(0.2), jnp.log(0.5))) / SEQUENCE_TOKENS
    decay_rates = jnp.where(slow_heads, slow_rate, fast_rate)
    n_devices = SEQUENCE_TOKENS // TOK_DEV
    dev_factor = jnp.exp(jax.random.uniform(key_dev, (n_devices,), jnp.float32, -0.69, 0.69))
    factor_row_list = jnp.repeat(dev_factor, TOK_DEV, total_repeat_length=SEQUENCE_TOKENS)
    cluster_position = jax.random.randint(key_position, (RETENTION_HEADS, 2), 0, SEQUENCE_TOKENS)
    cluster_depth = jax.random.uniform(key_level, (RETENTION_HEADS, 2), jnp.float32, -0.6, -0.22)
    matches = (jnp.arange(SEQUENCE_TOKENS)[None, None, :] == cluster_position[:, :, None]).astype(jnp.float32)
    clusters = jnp.sum(matches * cluster_depth[:, :, None], axis=1)
    return -decay_rates[:, None] * factor_row_list[None, :] + clusters


def levels(key, extent, shards, least, top_value):
    gain, own = 1.0, jax.random.fold_in(key, 6)
    for position, parts in shards:
        draws = jnp.exp(jax.random.uniform(jax.random.fold_in(own, position), (parts,), jnp.float32, least / len(shards), top_value / len(shards)))
        gain = gain * jnp.repeat(draws, extent[position] // parts).reshape([-1 if axis == position else 1 for axis in range(len(extent))])
    return gain


def scatter_about(stream_key, shape, spread, reach, pieces=(), kind=jnp.bfloat16):
    loudness = levels(stream_key, shape, pieces, -0.22, 0.18) if pieces else 1.0
    values = jax.random.normal(stream_key, shape, jnp.float32) * spread * loudness
    return jnp.minimum(jnp.maximum(values, -reach), reach).astype(kind)


def setup_inputs(seed: int = 0) -> dict:
    seeds = jax.random.split(jax.random.key(seed), 10)
    return {
        "tokens": scatter_about(seeds[0], (SEQUENCE_TOKENS, D), 1.0, 6.0, ((0, 16),)),
        "w_query": scatter_about(seeds[1], (D, RET_WIDTH), D ** -0.5, 0.125, ((1, 8),)),
        "w_key": scatter_about(seeds[2], (D, RET_WIDTH), D ** -0.5, 0.125, ((1, 8),)),
        "w_value": scatter_about(seeds[3], (D, RET_WIDTH), D ** -0.5, 0.125, ((1, 8),)),
        "w_gate": scatter_about(seeds[4], (D, RET_WIDTH), D ** -0.5, 0.125, ((1, 8),)),
        "w_pool": scatter_about(seeds[5], (D, POOL_WIDTH), D ** -0.5, 0.125, ((1, 8),)),
        "norm_gain": jnp.clip(1.0 + 0.18 * jax.random.normal(seeds[6], (RET_WIDTH,), jnp.float32), 0.1, 1.9),
        "log_decay": draw_log_decay(jax.random.fold_in(seeds[9], 71), 0),
        "w_out": scatter_about(seeds[8], (RET_WIDTH + POOL_WIDTH, D), (RET_WIDTH + POOL_WIDTH) ** -0.5, 0.125),
    }


def rotate(tensor, positions):
    half_dim = tensor.shape[-1] // 2
    inverse = 10000.0 ** (-jnp.arange(half_dim, dtype=jnp.float32) / half_dim)
    angles = positions.astype(jnp.float32)[:, None] * inverse[None, :]
    cosine = jnp.cos(angles)[:, None, :]
    sine_part = jnp.sin(angles)[:, None, :]
    first_half = tensor[..., :half_dim]
    second_half = tensor[..., half_dim:]
    return jnp.concatenate([first_half * cosine - second_half * sine_part, first_half * sine_part + second_half * cosine], axis=-1)

def block_parts(q_blocks, k_blocks, v_blocks, decay_blocks):
    log_cum = jnp.cumsum(decay_blocks, axis=1)
    block_ends = log_cum[:, -1, :]
    steps_len = q_blocks.shape[1]
    causal = jnp.arange(steps_len)[:, None] >= jnp.arange(steps_len)[None, :]
    head_cum = jnp.transpose(log_cum, (0, 2, 1))
    log_gap = head_cum[:, :, :, None] - head_cum[:, :, None, :]
    weights = jnp.where(causal[None, None], jnp.exp(jnp.minimum(log_gap, 0.0)), 0.0)
    scores = jnp.einsum('nthd,nshd->nhts', q_blocks.astype(jnp.float32), k_blocks.astype(jnp.float32))
    mixing = (scores * weights).astype(jnp.bfloat16)
    inner_part = jnp.einsum('nhts,nshe->nthe', mixing.astype(jnp.float32), v_blocks.astype(jnp.float32))
    keys_decayed = (k_blocks.astype(jnp.float32) * jnp.exp(block_ends[:, None, :] - log_cum)[..., None]).astype(jnp.bfloat16)
    updates = jnp.einsum('nshd,nshe->nhde', keys_decayed.astype(jnp.float32), v_blocks.astype(jnp.float32))
    return (log_cum, block_ends, inner_part, updates)

def reference(tokens, w_query, w_key, w_value, w_gate, w_pool, norm_gain, log_decay, w_out):

    def project(weights):
        return jnp.dot(tokens, weights, preferred_element_type=jnp.float32).astype(jnp.bfloat16)
    query = project(w_query)
    keys_raw = project(w_key)
    values = project(w_value)
    gate_pre = project(w_gate)
    pool_in = project(w_pool)
    positions = jnp.arange(SEQUENCE_TOKENS)
    head_shape = (SEQUENCE_TOKENS, RETENTION_HEADS, HEAD_DIM)
    q_rot = rotate(query.astype(jnp.float32).reshape(head_shape), positions).astype(jnp.bfloat16)
    k_rot = (rotate(keys_raw.astype(jnp.float32).reshape(head_shape), positions) * HEAD_DIM ** (-0.5)).astype(jnp.bfloat16)
    n_blocks = SEQUENCE_TOKENS // BLOCK
    block_shape = (n_blocks, BLOCK, RETENTION_HEADS, HEAD_DIM)
    q_blocks = q_rot.reshape(block_shape)
    k_blocks = k_rot.reshape(block_shape)
    v_blocks = values.reshape(block_shape)
    decay_blocks = jnp.transpose(log_decay).reshape(n_blocks, BLOCK, RETENTION_HEADS)
    log_cum, block_ends, inner_part, updates = block_parts(q_blocks, k_blocks, v_blocks, decay_blocks)

    def advance(running, element):
        block_end, update_n = element
        return (running * jnp.exp(block_end)[:, None, None] + update_n, running)
    zero_state = jnp.zeros((RETENTION_HEADS, HEAD_DIM, HEAD_DIM), jnp.float32)
    _, before_state = lax.scan(advance, zero_state, (block_ends, updates))
    state_bf = lax.optimization_barrier(before_state.astype(jnp.bfloat16))
    cross_part = jnp.einsum('nthd,nhde->nthe', q_blocks.astype(jnp.float32), state_bf.astype(jnp.float32)) * jnp.exp(log_cum)[..., None]
    retained = (inner_part + cross_part).reshape(head_shape)
    centered = retained - lax.optimization_barrier(jnp.mean(retained, axis=-1, keepdims=True))
    normed = centered * lax.rsqrt(lax.optimization_barrier(jnp.mean(centered * centered, axis=-1, keepdims=True)) + 1e-06)
    gated = (jax.nn.silu(gate_pre.astype(jnp.float32)) * norm_gain * normed.reshape(SEQUENCE_TOKENS, RET_WIDTH)).astype(jnp.bfloat16)
    filled = pool_in.astype(jnp.float32)
    prefix = jnp.concatenate([jnp.zeros((1, POOL_WIDTH), jnp.float32), jnp.cumsum(filled, axis=0)], axis=0)
    col_group = jnp.arange(POOL_WIDTH) // POOL_GROUP
    counts_base = (jnp.arange(SEQUENCE_TOKENS) + 1).astype(jnp.float32)[:, None]
    selected = jnp.zeros((SEQUENCE_TOKENS, POOL_WIDTH), jnp.float32)
    for group_idx in range(4):
        window_len = 2 ** (group_idx + 1)
        lower_sum = jnp.concatenate([jnp.zeros((window_len - 1, POOL_WIDTH), jnp.float32), prefix[:SEQUENCE_TOKENS + 1 - window_len]], axis=0)
        window_mean = (prefix[1:] - lower_sum) / jnp.minimum(counts_base, float(window_len))
        selected = jnp.where((col_group == group_idx)[None, :], window_mean, selected)
    pooled = (selected - filled).astype(jnp.bfloat16)
    result = jnp.dot(gated, w_out[:RET_WIDTH], preferred_element_type=jnp.float32) + jnp.dot(pooled, w_out[RET_WIDTH:], preferred_element_type=jnp.float32)
    return result.astype(jnp.bfloat16)
```

```python
import functools

import jax
import jax.numpy as jnp
import numpy as np
from jax import lax
from jax.experimental import pallas as pl
from jax.experimental.pallas import tpu as pltpu
from jax.sharding import PartitionSpec as P

HEAD = 128
CHUNK = 256
HALO = 16
F32 = jnp.float32
BF16 = jnp.bfloat16
VMEM_LIMIT = 63 * 1024 * 1024


def dot(a, b):
    return jnp.dot(a, b, preferred_element_type=F32)


def dot_nt(a, b):
    return lax.dot_general(a, b, (((1,), (1,)), ((), ())), preferred_element_type=F32)


def dot_tn(a, b):
    return lax.dot_general(a, b, (((0,), (0,)), ((), ())), preferred_element_type=F32)


def angle_tables(positions):
    half = HEAD // 2
    inverse = 10000.0 ** (-np.arange(half, dtype=np.float64) / half)
    angles = np.asarray(positions, np.float64)[:, None] * inverse[None, :]
    cosine, sine = np.cos(angles), np.sin(angles)
    return (
        np.concatenate([cosine, cosine], axis=1).astype(np.float32),
        np.concatenate([-sine, sine], axis=1).astype(np.float32),
    )


def lane_cumsum(x):
    lane = lax.broadcasted_iota(jnp.int32, x.shape, 1)
    step = 1
    while step < x.shape[1]:
        x = x + jnp.where(lane >= step, pltpu.roll(x, step, 1), 0.0)
        step *= 2
    return x


def kernel(
    n_sp,
    n_tp,
    tok_hbm,
    wq_hbm,
    wk_hbm,
    wv_hbm,
    wg_hbm,
    wp_hbm,
    gain_hbm,
    ld_hbm,
    wout_hbm,
    fine_hbm,
    base_hbm,
    out_hbm,
    x_ref,
    wkv_ref,
    wqg_ref,
    wp_ref,
    wout_ref,
    gain_ref,
    ld_ref,
    fine_ref,
    base_ref,
    k_ref,
    v_ref,
    q_ref,
    g_ref,
    p_ref,
    halo_ref,
    halo_send,
    acc_ref,
    kcol_ref,
    ecol_ref,
    crow_ref,
    ccol_ref,
    be_ref,
    pre_ref,
    state_ref,
    sloc_ref,
    ssend_ref,
    srecv_ref,
    tsend_ref,
    trecv_ref,
    inc_ref,
    psend_ref,
    gsend_ref,
    prow_ref,
    grow_ref,
    oacc_ref,
    obuf_ref,
    tok_sem,
    in_sem,
    wout_sem,
    out_sem,
    tsend_sem,
    trecv_sem,
    ssend_sem,
    srecv_sem,
    hsend_sem,
    hrecv_sem,
    psend_sem,
    precv_sem,
    gsend_sem,
    grecv_sem,
):
    sp = lax.axis_index("sp")
    tp = lax.axis_index("tp")
    rows = x_ref.shape[0]
    n_ch = rows // CHUNK
    width = wout_ref.shape[0] // 2
    n_x = n_tp // 2

    barrier = pltpu.get_barrier_semaphore()
    for j in range(1, n_sp):
        pl.semaphore_signal(barrier, inc=1, device_id={"sp": lax.rem(sp + j, n_sp)})
    for j in range(1, n_tp):
        pl.semaphore_signal(barrier, inc=1, device_id={"tp": lax.rem(tp + j, n_tp)})

    small = [
        pltpu.make_async_copy(ld_hbm, ld_ref, in_sem.at[0]),
        pltpu.make_async_copy(fine_hbm, fine_ref, in_sem.at[1]),
        pltpu.make_async_copy(
            base_hbm.at[:, pl.ds(pl.multiple_of(sp * n_ch, n_ch), n_ch), :], base_ref, in_sem.at[2]
        ),
        pltpu.make_async_copy(gain_hbm, gain_ref, in_sem.at[3]),
    ]
    w_copies = [
        pltpu.make_async_copy(wk_hbm, wkv_ref.at[:, 0:HEAD], in_sem.at[4]),
        pltpu.make_async_copy(wv_hbm, wkv_ref.at[:, HEAD : 2 * HEAD], in_sem.at[5]),
        pltpu.make_async_copy(wp_hbm, wp_ref, in_sem.at[6]),
        pltpu.make_async_copy(wq_hbm, wqg_ref.at[:, 0:HEAD], in_sem.at[7]),
        pltpu.make_async_copy(wg_hbm, wqg_ref.at[:, HEAD : 2 * HEAD], in_sem.at[8]),
    ]

    def chunk_of(c):
        return pl.ds(pl.multiple_of(c * CHUNK, CHUNK), CHUNK)

    def tok_copy(c):
        return pltpu.make_async_copy(
            tok_hbm.at[chunk_of(c), :], x_ref.at[chunk_of(c), :], tok_sem.at[c]
        )

    wout_copy = pltpu.make_async_copy(wout_hbm, wout_ref, wout_sem)

    for copy in small:
        copy.start()
    w_copies[0].start()
    w_copies[1].start()
    for c in range(n_ch):
        tok_copy(c).start()
    for copy in w_copies[2:]:
        copy.start()
    wout_copy.start()

    small[0].wait()
    lc = lane_cumsum(ld_ref[...])
    lct = jnp.transpose(lc)
    run = jnp.zeros((1, 1), F32)
    for c in range(n_ch):
        a, b = 2 * c, 2 * c + 1
        end_a = lc[a : a + 1, HEAD - 1 :]
        end = end_a + lc[b : b + 1, HEAD - 1 :]
        crow_ref[c, 0:1, :] = jnp.concatenate([lc[a : a + 1, :], lc[b : b + 1, :] + end_a], axis=1)
        col = jnp.concatenate(
            [
                jnp.broadcast_to(lct[:, a : a + 1], (HEAD, HEAD)),
                jnp.broadcast_to(lct[:, b : b + 1] + end_a, (HEAD, HEAD)),
            ],
            axis=0,
        )
        here = slice(c * CHUNK, (c + 1) * CHUNK)
        ccol_ref[here, :] = col
        kcol_ref[here, :] = jnp.exp(end - col)
        ecol_ref[here, :] = jnp.exp(col)
        be_ref[c : c + 1, :] = jnp.broadcast_to(jnp.exp(end), (1, HEAD))
        pre_ref[c : c + 1, :] = jnp.broadcast_to(jnp.exp(run), (1, HEAD))
        run = run + end
    tsend_ref[...] = jnp.broadcast_to(run, tsend_ref.shape)

    pl.semaphore_wait(barrier, n_sp - 1 + n_tp - 1)

    def t_copy(j):
        return pltpu.make_async_remote_copy(
            src_ref=tsend_ref,
            dst_ref=trecv_ref.at[sp],
            send_sem=tsend_sem.at[j],
            recv_sem=trecv_sem.at[sp],
            device_id={"sp": lax.rem(sp + j, n_sp)},
            device_id_type=pl.DeviceIdType.MESH,
        )

    def s_copy(j):
        return pltpu.make_async_remote_copy(
            src_ref=ssend_ref,
            dst_ref=srecv_ref.at[sp],
            send_sem=ssend_sem.at[j],
            recv_sem=srecv_sem.at[sp],
            device_id={"sp": lax.rem(sp + j, n_sp)},
            device_id_type=pl.DeviceIdType.MESH,
        )

    for j in range(1, n_sp):

        @pl.when(sp + j < n_sp)
        def _():
            t_copy(j).start()

    small[1].wait()
    small[2].wait()
    w_copies[0].wait()
    w_copies[1].wait()
    state_ref[...] = jnp.zeros_like(state_ref)

    def turned(x, c):
        base_c = base_ref[0, pl.ds(c, 1), :]
        base_s = base_ref[1, pl.ds(c, 1), :]
        fine_c = fine_ref[0]
        fine_s = fine_ref[1]
        cosine = base_c * fine_c - base_s * fine_s
        sine = base_s * fine_c + base_c * fine_s
        return x * cosine + pltpu.roll(x, HEAD // 2, 1) * sine

    def kv_step(c, carry):
        tok_copy(c).wait()
        here = chunk_of(c)
        kv = dot(x_ref[here, :], wkv_ref[...])
        key = kv[:, :HEAD].astype(BF16).astype(F32)
        value = kv[:, HEAD:].astype(BF16)
        k_rot = (turned(key, c) * HEAD**-0.5).astype(BF16)
        k_ref[here, :] = k_rot
        v_ref[here, :] = value
        decayed = (k_rot.astype(F32) * kcol_ref[here, :]).astype(BF16)
        update = dot_tn(decayed, value)
        state = state_ref[...]
        sloc_ref[c] = state.astype(BF16)
        state_ref[...] = state * be_ref[pl.ds(c, 1), :] + update
        return carry

    lax.fori_loop(0, n_ch, kv_step, 0)
    ssend_ref[...] = state_ref[...].astype(BF16)
    for j in range(1, n_sp):

        @pl.when(sp + j < n_sp)
        def _():
            s_copy(j).start()

    w_copies[2].wait()

    def p_of(c):
        here = chunk_of(c)
        p = dot(x_ref[here, :], wp_ref[...]).astype(BF16)
        p_ref[pl.ds(pl.multiple_of(HALO + c * CHUNK, HALO), CHUNK), :] = p.astype(F32)
        return p

    halo_copy = pltpu.make_async_remote_copy(
        src_ref=halo_send,
        dst_ref=halo_ref,
        send_sem=hsend_sem,
        recv_sem=hrecv_sem,
        device_id={"sp": lax.rem(sp + 1, n_sp)},
        device_id_type=pl.DeviceIdType.MESH,
    )
    halo_send[...] = p_of(n_ch - 1)[CHUNK - HALO :, :]

    @pl.when(sp + 1 < n_sp)
    def _():
        halo_copy.start()

    def p_step(c, carry):
        p_of(c)
        return carry

    lax.fori_loop(0, n_ch - 1, p_step, 0)

    @pl.when(sp > 0)
    def _():
        halo_copy.wait_recv()
        p_ref[0:HALO, :] = halo_ref[...].astype(F32)

    @pl.when(sp == 0)
    def _():
        p_ref[0:HALO, :] = jnp.zeros((HALO, HEAD), F32)

    x_at, core = lax.div(tp, 2), lax.rem(tp, 2)
    order = [(2, 0), (3, 0), (2, 1), (3, 1), (1, 0), (1, 1), (0, 1), (0, 0)]

    def peer_of(dx, dc):
        return lax.rem(x_at + dx, n_x) * 2 + lax.rem(core + dc, 2)

    def row_copy(k, send_ref, recv_ref, send_sem, recv_sem):
        peer = peer_of(*order[k])
        return pltpu.make_async_remote_copy(
            src_ref=send_ref.at[peer],
            dst_ref=recv_ref.at[tp],
            send_sem=send_sem.at[k],
            recv_sem=recv_sem.at[tp],
            device_id={"tp": peer},
            device_id_type=pl.DeviceIdType.MESH,
        )

    def recv_wait(j, send_ref, recv_ref, send_sem, recv_sem):
        pltpu.make_async_remote_copy(
            src_ref=send_ref.at[0],
            dst_ref=recv_ref.at[j],
            send_sem=send_sem.at[0],
            recv_sem=recv_sem.at[j],
            device_id={"tp": tp},
            device_id_type=pl.DeviceIdType.MESH,
        ).wait_recv()

    group = lax.div(tp * HEAD, 256)
    window = jnp.left_shift(jnp.int32(2), group)

    def pooled_of(c):
        x = p_ref[pl.ds(pl.multiple_of(c * CHUNK, CHUNK), CHUNK + HALO), :]
        s = x + pltpu.roll(x, 1, 0)
        for level in (1, 2, 3):
            s = jnp.where(group >= level, s + pltpu.roll(s, 2**level, 0), s)
        s = s[HALO:, :]
        x = x[HALO:, :]
        at = lax.broadcasted_iota(jnp.int32, (HALO, HEAD), 0) + (sp * rows + c * CHUNK + 1)
        count = jnp.minimum(at, window).astype(F32)
        whole = jnp.minimum(lax.broadcasted_iota(jnp.int32, (1, HEAD), 1) + 4096, window).astype(F32)
        top = s[:HALO, :] / count
        rest = s[HALO:, :] * (1.0 / whole)
        return (jnp.concatenate([top, rest], axis=0) - x).astype(BF16)

    p_args = (psend_ref, prow_ref, psend_sem, precv_sem)
    g_args = (gsend_ref, grow_ref, gsend_sem, grecv_sem)
    for k in range(n_tp - 1):
        peer = peer_of(*order[k])
        psend_ref[peer] = pooled_of(peer)
        row_copy(k, *p_args).start()
    prow_ref[tp] = pooled_of(tp)

    w_copies[3].wait()
    w_copies[4].wait()
    tri = lax.broadcasted_iota(jnp.int32, (CHUNK, CHUNK), 0) >= lax.broadcasted_iota(
        jnp.int32, (CHUNK, CHUNK), 1
    )

    def q_step(c, carry):
        here = chunk_of(c)
        qg = dot(x_ref[here, :], wqg_ref[...])
        query = qg[:, :HEAD].astype(BF16).astype(F32)
        g_ref[here, :] = qg[:, HEAD:].astype(BF16)
        q_rot = turned(query, c).astype(BF16)
        q_ref[here, :] = q_rot
        scores = dot_nt(q_rot, k_ref[here, :])
        col = ccol_ref[here, :]
        gap = jnp.concatenate([col, col], axis=1) - crow_ref[c, 0:1, :]
        weights = jnp.where(tri, jnp.exp(jnp.minimum(gap, 0.0)), 0.0)
        mixing = (scores * weights).astype(BF16)
        inner = dot(mixing, v_ref[here, :])
        cross = dot(q_rot, sloc_ref[c]) * ecol_ref[here, :]
        acc_ref[here, :] = inner + cross
        return carry

    lax.fori_loop(0, n_ch, q_step, 0)

    inc_ref[...] = jnp.zeros_like(inc_ref)

    def inc_step(j, carry):
        t_wait = pltpu.make_async_remote_copy(
            src_ref=tsend_ref,
            dst_ref=trecv_ref.at[j],
            send_sem=tsend_sem.at[0],
            recv_sem=trecv_sem.at[j],
            device_id={"sp": sp},
            device_id_type=pl.DeviceIdType.MESH,
        )
        s_wait = pltpu.make_async_remote_copy(
            src_ref=ssend_ref,
            dst_ref=srecv_ref.at[j],
            send_sem=ssend_sem.at[0],
            recv_sem=srecv_sem.at[j],
            device_id={"sp": sp},
            device_id_type=pl.DeviceIdType.MESH,
        )
        t_wait.wait_recv()
        s_wait.wait_recv()
        inc_ref[...] = inc_ref[...] * jnp.exp(trecv_ref[j, 0:1, :]) + srecv_ref[j].astype(F32)
        return carry

    lax.fori_loop(0, sp, inc_step, 0)
    incoming = inc_ref[...].astype(BF16)

    small[3].wait()

    def gated_of(c):
        here = chunk_of(c)
        cross = dot(q_ref[here, :], incoming) * (ecol_ref[here, :] * pre_ref[pl.ds(c, 1), :])
        retained = acc_ref[here, :] + cross
        centered = retained - jnp.mean(retained, axis=-1, keepdims=True)
        scale = lax.rsqrt(jnp.mean(centered * centered, axis=-1, keepdims=True) + 1e-06)
        gate = g_ref[here, :].astype(F32)
        return (gate * jax.nn.sigmoid(gate) * gain_ref[...] * (centered * scale)).astype(BF16)

    for k in range(n_tp - 1):
        peer = peer_of(*order[k])
        gsend_ref[peer] = gated_of(peer)
        row_copy(k, *g_args).start()
    grow_ref[tp] = gated_of(tp)

    wout_copy.wait()
    for j in range(n_tp):

        @pl.when(tp != j)
        def _():
            recv_wait(j, *p_args)

    n_cols = wout_ref.shape[1]
    tile = 256
    pool_rows = jnp.concatenate([prow_ref[j] for j in range(n_tp)], axis=1)

    def pool_step(i, carry):
        at = pl.ds(pl.multiple_of(i * tile, tile), tile)
        oacc_ref[:, at] = dot(pool_rows, wout_ref[pl.ds(width, width), at])
        return carry

    lax.fori_loop(0, n_cols // tile, pool_step, 0)

    def out_copy(i):
        at = pl.ds(pl.multiple_of(i * tile, tile), tile)
        return pltpu.make_async_copy(obuf_ref.at[:, at], out_hbm.at[:, at], out_sem.at[i])

    for n, dx in enumerate((0, 1, 3, 2)):
        pair = lax.rem(x_at + dx, n_x)
        if dx == 0:
            recv_wait(pair * 2 + 1 - core, *g_args)
        else:
            recv_wait(pair * 2, *g_args)
            recv_wait(pair * 2 + 1, *g_args)
        lhs = jnp.concatenate([grow_ref[pair * 2], grow_ref[pair * 2 + 1]], axis=1)
        deep = pl.ds(pl.multiple_of(pair * 2 * HEAD, 2 * HEAD), 2 * HEAD)

        def out_step(i, carry):
            at = pl.ds(pl.multiple_of(i * tile, tile), tile)
            total = oacc_ref[:, at] + dot(lhs, wout_ref[deep, at])
            if n < 3:
                oacc_ref[:, at] = total
            else:
                obuf_ref[:, at] = total.astype(BF16)
                out_copy(i).start()
            return carry

        lax.fori_loop(0, n_cols // tile, out_step, 0)

    for j in range(1, n_sp):

        @pl.when(sp + j < n_sp)
        def _():
            t_copy(j).wait_send()
            s_copy(j).wait_send()

    @pl.when(sp + 1 < n_sp)
    def _():
        halo_copy.wait_send()

    for k in range(n_tp - 1):
        row_copy(k, *p_args).wait_send()
        row_copy(k, *g_args).wait_send()
    for i in range(n_cols // tile):
        out_copy(i).wait()


def local(n_sp, n_tp, tokens, w_query, w_key, w_value, w_gate, w_pool, norm_gain, log_decay, w_out):
    rows, depth = tokens.shape
    n_ch = rows // CHUNK
    out_rows, out_cols = rows // n_tp, w_out.shape[1]
    fine = np.stack(angle_tables(np.arange(CHUNK)))
    base = np.stack(angle_tables(np.arange(n_sp * n_ch) * CHUNK))
    any_spec = pl.BlockSpec(memory_space=pl.ANY)
    dma = pltpu.SemaphoreType.DMA
    vm = pltpu.VMEM
    return pl.pallas_call(
        functools.partial(kernel, n_sp, n_tp),
        out_shape=jax.ShapeDtypeStruct((out_rows, out_cols), BF16),
        in_specs=[any_spec] * 11,
        out_specs=any_spec,
        scratch_shapes=[
            vm((rows, depth), BF16),
            vm((depth, 2 * HEAD), BF16),
            vm((depth, 2 * HEAD), BF16),
            vm((depth, HEAD), BF16),
            vm(w_out.shape, BF16),
            vm((1, HEAD), F32),
            vm((rows // HEAD, HEAD), F32),
            vm((2, CHUNK, HEAD), F32),
            vm((2, n_ch, HEAD), F32),
            vm((rows, HEAD), BF16),
            vm((rows, HEAD), BF16),
            vm((rows, HEAD), BF16),
            vm((rows, HEAD), BF16),
            vm((rows + HALO, HEAD), F32),
            vm((HALO, HEAD), BF16),
            vm((HALO, HEAD), BF16),
            vm((rows, HEAD), F32),
            vm((rows, HEAD), F32),
            vm((rows, HEAD), F32),
            vm((n_ch, 8, CHUNK), F32),
            vm((rows, HEAD), F32),
            vm((n_ch, HEAD), F32),
            vm((n_ch, HEAD), F32),
            vm((HEAD, HEAD), F32),
            vm((n_ch, HEAD, HEAD), BF16),
            vm((HEAD, HEAD), BF16),
            vm((n_sp, HEAD, HEAD), BF16),
            vm((8, HEAD), F32),
            vm((n_sp, 8, HEAD), F32),
            vm((HEAD, HEAD), F32),
            vm((n_tp, CHUNK, HEAD), BF16),
            vm((n_tp, CHUNK, HEAD), BF16),
            vm((n_tp, CHUNK, HEAD), BF16),
            vm((n_tp, CHUNK, HEAD), BF16),
            vm((out_rows, out_cols), F32),
            vm((out_rows, out_cols), BF16),
            dma((n_ch,)),
            dma((9,)),
            dma,
            dma((out_cols // 256,)),
            dma((n_sp,)),
            dma((n_sp,)),
            dma((n_sp,)),
            dma((n_sp,)),
            dma,
            dma,
            dma((n_tp,)),
            dma((n_tp,)),
            dma((n_tp,)),
            dma((n_tp,)),
        ],
        compiler_params=pltpu.CompilerParams(
            collective_id=0, has_side_effects=True, vmem_limit_bytes=VMEM_LIMIT
        ),
        name="layer",
    )(
        tokens,
        w_query,
        w_key,
        w_value,
        w_gate,
        w_pool,
        norm_gain.reshape(1, HEAD),
        log_decay.reshape(rows // HEAD, HEAD),
        w_out,
        fine,
        base,
    )


def solution(mesh):
    in_specs = (
        P("sp", None),
        P(None, "tp"),
        P(None, "tp"),
        P(None, "tp"),
        P(None, "tp"),
        P(None, "tp"),
        P("tp"),
        P("tp", "sp"),
        P(),
    )
    body = functools.partial(local, mesh.shape["sp"], mesh.shape["tp"])
    return jax.shard_map(
        body, mesh=mesh, in_specs=in_specs, out_specs=P(("sp", "tp"), None), check_vma=False
    )
```

```python
import functools

import jax
import jax.numpy as jnp
import numpy as np
from jax import lax
from jax.experimental import pallas as pl
from jax.experimental.pallas import tpu as pltpu
from jax.sharding import PartitionSpec as P

HEAD = 128
CHUNK = 256
HALO = 16
F32 = jnp.float32
BF16 = jnp.bfloat16
VMEM_LIMIT = 62 * 1024 * 1024 + 512 * 1024


def dot(a, b):
    return jnp.dot(a, b, preferred_element_type=F32)


def dot_nt(a, b):
    return lax.dot_general(a, b, (((1,), (1,)), ((), ())), preferred_element_type=F32)


def dot_tn(a, b):
    return lax.dot_general(a, b, (((0,), (0,)), ((), ())), preferred_element_type=F32)


def angle_tables(positions):
    half = HEAD // 2
    inverse = 10000.0 ** (-np.arange(half, dtype=np.float64) / half)
    angles = np.asarray(positions, np.float64)[:, None] * inverse[None, :]
    cosine, sine = np.cos(angles), np.sin(angles)
    return (
        np.concatenate([cosine, cosine], axis=1).astype(np.float32),
        np.concatenate([-sine, sine], axis=1).astype(np.float32),
    )


def lane_cumsum(x):
    lane = lax.broadcasted_iota(jnp.int32, x.shape, 1)
    step = 1
    while step < x.shape[1]:
        x = x + jnp.where(lane >= step, pltpu.roll(x, step, 1), 0.0)
        step *= 2
    return x


def kernel(
    n_sp,
    n_tp,
    tok_hbm,
    wq_hbm,
    wk_hbm,
    wv_hbm,
    wg_hbm,
    wp_hbm,
    gain_hbm,
    ld_hbm,
    wout_hbm,
    fine_hbm,
    base_hbm,
    obuf_ref,
    x_ref,
    wkv_ref,
    wqg_ref,
    wp_ref,
    wout_ref,
    gain_ref,
    ld_ref,
    fine_ref,
    base_ref,
    k_ref,
    v_ref,
    q_ref,
    g_ref,
    p_ref,
    halo_ref,
    halo_send,
    acc_ref,
    kcol_ref,
    ecol_ref,
    crow_ref,
    ccol_ref,
    be_ref,
    pre_ref,
    sloc_ref,
    ssend_ref,
    srecv_ref,
    tsend_ref,
    trecv_ref,
    inc_ref,
    psend_ref,
    gsend_ref,
    prow_ref,
    grow_ref,
    oacc_ref,
    tok_sem,
    in_sem,
    wout_sem,
    tsend_sem,
    trecv_sem,
    ssend_sem,
    srecv_sem,
    hsend_sem,
    hrecv_sem,
    psend_sem,
    precv_sem,
    gsend_sem,
    grecv_sem,
):
    sp = lax.axis_index("sp")
    tp = lax.axis_index("tp")
    rows = x_ref.shape[0]
    n_ch = rows // CHUNK
    width = wout_ref.shape[0] // 2
    n_x = n_tp // 2

    barrier = pltpu.get_barrier_semaphore()
    for j in range(1, n_sp):
        pl.semaphore_signal(barrier, inc=1, device_id={"sp": lax.rem(sp + j, n_sp)})
    for j in range(1, n_tp):
        pl.semaphore_signal(barrier, inc=1, device_id={"tp": lax.rem(tp + j, n_tp)})

    small = [
        pltpu.make_async_copy(ld_hbm, ld_ref, in_sem.at[0]),
        pltpu.make_async_copy(fine_hbm, fine_ref, in_sem.at[1]),
        pltpu.make_async_copy(
            base_hbm.at[:, pl.ds(pl.multiple_of(sp * n_ch, n_ch), n_ch), :], base_ref, in_sem.at[2]
        ),
        pltpu.make_async_copy(gain_hbm, gain_ref, in_sem.at[3]),
    ]
    w_copies = [
        pltpu.make_async_copy(wk_hbm, wkv_ref.at[:, 0:HEAD], in_sem.at[4]),
        pltpu.make_async_copy(wv_hbm, wkv_ref.at[:, HEAD : 2 * HEAD], in_sem.at[5]),
        pltpu.make_async_copy(wp_hbm, wp_ref, in_sem.at[6]),
        pltpu.make_async_copy(wq_hbm, wqg_ref.at[:, 0:HEAD], in_sem.at[7]),
        pltpu.make_async_copy(wg_hbm, wqg_ref.at[:, HEAD : 2 * HEAD], in_sem.at[8]),
    ]

    def chunk_of(c):
        if isinstance(c, int):
            return slice(c * CHUNK, (c + 1) * CHUNK)
        return pl.ds(pl.multiple_of(c * CHUNK, CHUNK), CHUNK)

    def tok_copy(c):
        return pltpu.make_async_copy(
            tok_hbm.at[chunk_of(c), :], x_ref.at[chunk_of(c), :], tok_sem.at[c]
        )

    wout_copy = pltpu.make_async_copy(wout_hbm, wout_ref, wout_sem)

    small[0].start()
    w_copies[0].start()
    w_copies[1].start()
    small[1].start()
    small[2].start()
    for c in range(n_ch):
        tok_copy(c).start()

    small[0].wait()
    lc = lane_cumsum(ld_ref[...])
    lct = jnp.transpose(lc)
    run = jnp.zeros((1, 1), F32)
    for c in range(n_ch):
        a, b = 2 * c, 2 * c + 1
        end_a = lc[a : a + 1, HEAD - 1 :]
        end = end_a + lc[b : b + 1, HEAD - 1 :]
        crow_ref[c, 0:1, :] = jnp.concatenate([lc[a : a + 1, :], lc[b : b + 1, :] + end_a], axis=1)
        col = jnp.concatenate(
            [
                jnp.broadcast_to(lct[:, a : a + 1], (HEAD, HEAD)),
                jnp.broadcast_to(lct[:, b : b + 1] + end_a, (HEAD, HEAD)),
            ],
            axis=0,
        )
        here = slice(c * CHUNK, (c + 1) * CHUNK)
        ccol_ref[here, :] = col
        kcol_ref[here, :] = jnp.exp(end - col)
        ecol_ref[here, :] = jnp.exp(col)
        be_ref[c : c + 1, :] = jnp.broadcast_to(jnp.exp(end), (1, HEAD))
        pre_ref[c : c + 1, :] = jnp.broadcast_to(jnp.exp(run), (1, HEAD))
        run = run + end
    tsend_ref[...] = jnp.broadcast_to(run, tsend_ref.shape)

    def t_copy(j):
        return pltpu.make_async_remote_copy(
            src_ref=tsend_ref,
            dst_ref=trecv_ref.at[sp],
            send_sem=tsend_sem.at[j],
            recv_sem=trecv_sem.at[sp],
            device_id={"sp": lax.rem(sp + j, n_sp)},
            device_id_type=pl.DeviceIdType.MESH,
        )

    def s_copy(j):
        return pltpu.make_async_remote_copy(
            src_ref=ssend_ref,
            dst_ref=srecv_ref.at[sp],
            send_sem=ssend_sem.at[j],
            recv_sem=srecv_sem.at[sp],
            device_id={"sp": lax.rem(sp + j, n_sp)},
            device_id_type=pl.DeviceIdType.MESH,
        )

    small[1].wait()
    small[2].wait()
    w_copies[0].wait()
    w_copies[1].wait()

    def turned(x, c):
        base_c = base_ref[0, pl.ds(c, 1), :]
        base_s = base_ref[1, pl.ds(c, 1), :]
        fine_c = fine_ref[0]
        fine_s = fine_ref[1]
        cosine = base_c * fine_c - base_s * fine_s
        sine = base_s * fine_c + base_c * fine_s
        return x * cosine + pltpu.roll(x, HEAD // 2, 1) * sine

    def kv_of(c):
        if c % 2 == 0:
            tok_copy(c).wait()
            tok_copy(c + 1).wait()
        if c == 4:
            for copy in w_copies[2:]:
                copy.start()
            small[3].start()
        return dot(x_ref[chunk_of(c), :], wkv_ref[...])

    def keep_kv(c, kv, state):
        here = chunk_of(c)
        key = kv[:, :HEAD].astype(BF16).astype(F32)
        value = kv[:, HEAD:].astype(BF16)
        k_rot = (turned(key, c) * HEAD**-0.5).astype(BF16)
        k_ref[here, :] = k_rot
        v_ref[here, :] = value
        decayed = (k_rot.astype(F32) * kcol_ref[here, :]).astype(BF16)
        update = dot_tn(decayed, value)
        sloc_ref[c] = state.astype(BF16)
        return state * be_ref[pl.ds(c, 1), :] + update

    state = jnp.zeros((HEAD, HEAD), F32)
    kv = kv_of(0)
    for c in range(n_ch):
        if c + 1 < n_ch:
            kv_next = kv_of(c + 1)
        state = keep_kv(c, kv, state)
        kv = kv_next
    wout_copy.start()
    ssend_ref[...] = state.astype(BF16)

    pl.semaphore_wait(barrier, n_sp - 1 + n_tp - 1)
    for j in range(1, n_sp):

        @pl.when(sp + j < n_sp)
        def _():
            t_copy(j).start()
            s_copy(j).start()

    w_copies[2].wait()

    def p_of(c):
        here = chunk_of(c)
        p = dot(x_ref[here, :], wp_ref[...]).astype(BF16)
        p_ref[HALO + c * CHUNK : HALO + (c + 1) * CHUNK, :] = p.astype(F32)
        return p

    halo_copy = pltpu.make_async_remote_copy(
        src_ref=halo_send,
        dst_ref=halo_ref,
        send_sem=hsend_sem,
        recv_sem=hrecv_sem,
        device_id={"sp": lax.rem(sp + 1, n_sp)},
        device_id_type=pl.DeviceIdType.MESH,
    )
    p_ref[0:HALO, :] = jnp.zeros((HALO, HEAD), F32)
    halo_send[...] = p_of(n_ch - 1)[CHUNK - HALO :, :]

    @pl.when(sp + 1 < n_sp)
    def _():
        halo_copy.start()

    for c in range(n_ch - 1):
        p_of(c)

    x_at, core = lax.div(tp, 2), lax.rem(tp, 2)
    order = [(2, 0), (3, 0), (2, 1), (3, 1), (1, 0), (1, 1), (0, 1), (0, 0)]

    def peer_of(dx, dc):
        return lax.rem(x_at + dx, n_x) * 2 + lax.rem(core + dc, 2)

    def row_copy(peer, send_ref, recv_ref, send_sem, recv_sem):
        return pltpu.make_async_remote_copy(
            src_ref=send_ref.at[peer],
            dst_ref=recv_ref.at[tp],
            send_sem=send_sem.at[peer],
            recv_sem=recv_sem.at[tp],
            device_id={"tp": peer},
            device_id_type=pl.DeviceIdType.MESH,
        )

    def recv_wait(j, send_ref, recv_ref, send_sem, recv_sem):
        pltpu.make_async_remote_copy(
            src_ref=send_ref.at[0],
            dst_ref=recv_ref.at[j],
            send_sem=send_sem.at[0],
            recv_sem=recv_sem.at[j],
            device_id={"tp": tp},
            device_id_type=pl.DeviceIdType.MESH,
        ).wait_recv()

    group = lax.div(tp * HEAD, 256)
    window = jnp.left_shift(jnp.int32(2), group)

    def pooled_of(c):
        x = p_ref[pl.ds(pl.multiple_of(c * CHUNK, CHUNK), CHUNK + HALO), :]
        s = x + pltpu.roll(x, 1, 0)
        for level in (1, 2, 3):
            s = jnp.where(group >= level, s + pltpu.roll(s, 2**level, 0), s)
        s = s[HALO:, :]
        x = x[HALO:, :]
        at = lax.broadcasted_iota(jnp.int32, (HALO, HEAD), 0) + (sp * rows + c * CHUNK + 1)
        count = jnp.minimum(at, window).astype(F32)
        whole = jnp.minimum(lax.broadcasted_iota(jnp.int32, (1, HEAD), 1) + 4096, window).astype(F32)
        top = s[:HALO, :] / count
        rest = s[HALO:, :] * (1.0 / whole)
        return (jnp.concatenate([top, rest], axis=0) - x).astype(BF16)

    p_args = (psend_ref, prow_ref, psend_sem, precv_sem)
    g_args = (gsend_ref, grow_ref, gsend_sem, grecv_sem)
    for k in range(n_tp - 1):
        peer = peer_of(*order[k])
        psend_ref[peer] = pooled_of(peer)

        @pl.when(peer != 0)
        def _():
            row_copy(peer, *p_args).start()

    prow_ref[tp] = pooled_of(tp)

    w_copies[3].wait()
    w_copies[4].wait()
    tri = lax.broadcasted_iota(jnp.int32, (CHUNK, CHUNK), 0) >= lax.broadcasted_iota(
        jnp.int32, (CHUNK, CHUNK), 1
    )

    def keep_q(c, qg):
        here = chunk_of(c)
        query = qg[:, :HEAD].astype(BF16).astype(F32)
        g_ref[here, :] = qg[:, HEAD:].astype(BF16)
        q_rot = turned(query, c).astype(BF16)
        q_ref[here, :] = q_rot
        scores = dot_nt(q_rot, k_ref[here, :])
        col = ccol_ref[here, :]
        gap = jnp.concatenate([col, col], axis=1) - crow_ref[c, 0:1, :]
        weights = jnp.where(tri, jnp.exp(jnp.minimum(gap, 0.0)), 0.0)
        mixing = (scores * weights).astype(BF16)
        inner = dot(mixing, v_ref[here, :])
        cross = dot(q_rot, sloc_ref[c]) * ecol_ref[here, :]
        acc_ref[here, :] = inner + cross

    qg = dot(x_ref[chunk_of(0), :], wqg_ref[...])
    for c in range(n_ch):
        if c + 1 < n_ch:
            qg_next = dot(x_ref[chunk_of(c + 1), :], wqg_ref[...])
        keep_q(c, qg)
        qg = qg_next

    @pl.when(sp > 0)
    def _():
        halo_copy.wait_recv()
        p_ref[0:HALO, :] = halo_ref[...].astype(F32)
    first = pooled_of(0)

    @pl.when(tp == 0)
    def _():
        prow_ref[0] = first

    @pl.when(tp != 0)
    def _():
        psend_ref[0] = first
        row_copy(0, *p_args).start()

    inc_ref[...] = jnp.zeros_like(inc_ref)

    def inc_step(j, carry):
        t_wait = pltpu.make_async_remote_copy(
            src_ref=tsend_ref,
            dst_ref=trecv_ref.at[j],
            send_sem=tsend_sem.at[0],
            recv_sem=trecv_sem.at[j],
            device_id={"sp": sp},
            device_id_type=pl.DeviceIdType.MESH,
        )
        s_wait = pltpu.make_async_remote_copy(
            src_ref=ssend_ref,
            dst_ref=srecv_ref.at[j],
            send_sem=ssend_sem.at[0],
            recv_sem=srecv_sem.at[j],
            device_id={"sp": sp},
            device_id_type=pl.DeviceIdType.MESH,
        )
        t_wait.wait_recv()
        s_wait.wait_recv()
        inc_ref[...] = inc_ref[...] * jnp.exp(trecv_ref[j, 0:1, :]) + srecv_ref[j].astype(F32)
        return carry

    lax.fori_loop(0, sp, inc_step, 0)
    incoming = inc_ref[...].astype(BF16)

    small[3].wait()

    def gated_of(c):
        here = chunk_of(c)
        cross = dot(q_ref[here, :], incoming) * (ecol_ref[here, :] * pre_ref[pl.ds(c, 1), :])
        retained = acc_ref[here, :] + cross
        centered = retained - jnp.mean(retained, axis=-1, keepdims=True)
        scale = lax.rsqrt(jnp.mean(centered * centered, axis=-1, keepdims=True) + 1e-06)
        gate = g_ref[here, :].astype(F32)
        return (gate * jax.nn.sigmoid(gate) * gain_ref[...] * (centered * scale)).astype(BF16)

    for k in range(n_tp - 1):
        peer = peer_of(*order[k])
        gsend_ref[peer] = gated_of(peer)
        row_copy(peer, *g_args).start()
    grow_ref[tp] = gated_of(tp)

    wout_copy.wait()
    for j in range(n_tp):

        @pl.when(tp != j)
        def _():
            recv_wait(j, *p_args)

    n_cols = wout_ref.shape[1]
    tile = 256
    pool_rows = jnp.concatenate([prow_ref[j] for j in range(n_tp)], axis=1)

    def pool_step(i, carry):
        at = pl.ds(pl.multiple_of(i * tile, tile), tile)
        oacc_ref[:, at] = dot(pool_rows, wout_ref[pl.ds(width, width), at])
        return carry

    lax.fori_loop(0, n_cols // tile, pool_step, 0)

    for n, dx in enumerate((0, 2, 1, 3)):
        pair = lax.rem(x_at + dx, n_x)
        if dx == 0:
            recv_wait(pair * 2 + 1 - core, *g_args)
        else:
            recv_wait(pair * 2, *g_args)
            recv_wait(pair * 2 + 1, *g_args)
        lhs = jnp.concatenate([grow_ref[pair * 2], grow_ref[pair * 2 + 1]], axis=1)
        deep = pl.ds(pl.multiple_of(pair * 2 * HEAD, 2 * HEAD), 2 * HEAD)

        def out_step(i, carry):
            at = pl.ds(pl.multiple_of(i * tile, tile), tile)
            total = oacc_ref[:, at] + dot(lhs, wout_ref[deep, at])
            if n < 3:
                oacc_ref[:, at] = total
            else:
                obuf_ref[:, at] = total.astype(BF16)
            return carry

        lax.fori_loop(0, n_cols // tile, out_step, 0)

    for j in range(1, n_sp):

        @pl.when(sp + j < n_sp)
        def _():
            t_copy(j).wait_send()
            s_copy(j).wait_send()

    @pl.when(sp + 1 < n_sp)
    def _():
        halo_copy.wait_send()

    for k in range(n_tp - 1):
        peer = peer_of(*order[k])
        row_copy(peer, *p_args).wait_send()
        row_copy(peer, *g_args).wait_send()


def local(n_sp, n_tp, tokens, w_query, w_key, w_value, w_gate, w_pool, norm_gain, log_decay, w_out):
    rows, depth = tokens.shape
    n_ch = rows // CHUNK
    out_rows, out_cols = rows // n_tp, w_out.shape[1]
    fine = np.stack(angle_tables(np.arange(CHUNK)))
    base = np.stack(angle_tables(np.arange(n_sp * n_ch) * CHUNK))
    any_spec = pl.BlockSpec(memory_space=pltpu.HBM)
    dma = pltpu.SemaphoreType.DMA
    vm = pltpu.VMEM
    return pl.pallas_call(
        functools.partial(kernel, n_sp, n_tp),
        out_shape=pltpu.VMEM((out_rows, out_cols), BF16),
        in_specs=[any_spec] * 11,
        out_specs=pl.BlockSpec(memory_space=pltpu.VMEM),
        scratch_shapes=[
            vm((rows, depth), BF16),
            vm((depth, 2 * HEAD), BF16),
            vm((depth, 2 * HEAD), BF16),
            vm((depth, HEAD), BF16),
            vm(w_out.shape, BF16),
            vm((1, HEAD), F32),
            vm((rows // HEAD, HEAD), F32),
            vm((2, CHUNK, HEAD), F32),
            vm((2, n_ch, HEAD), F32),
            vm((rows, HEAD), BF16),
            vm((rows, HEAD), BF16),
            vm((rows, HEAD), BF16),
            vm((rows, HEAD), BF16),
            vm((rows + HALO, HEAD), F32),
            vm((HALO, HEAD), BF16),
            vm((HALO, HEAD), BF16),
            vm((rows, HEAD), F32),
            vm((rows, HEAD), F32),
            vm((rows, HEAD), F32),
            vm((n_ch, 8, CHUNK), F32),
            vm((rows, HEAD), F32),
            vm((n_ch, HEAD), F32),
            vm((n_ch, HEAD), F32),
            vm((n_ch, HEAD, HEAD), BF16),
            vm((HEAD, HEAD), BF16),
            vm((n_sp, HEAD, HEAD), BF16),
            vm((8, HEAD), F32),
            vm((n_sp, 8, HEAD), F32),
            vm((HEAD, HEAD), F32),
            vm((n_tp, CHUNK, HEAD), BF16),
            vm((n_tp, CHUNK, HEAD), BF16),
            vm((n_tp, CHUNK, HEAD), BF16),
            vm((n_tp, CHUNK, HEAD), BF16),
            vm((out_rows, out_cols), F32),
            dma((n_ch,)),
            dma((9,)),
            dma,
            dma((n_sp,)),
            dma((n_sp,)),
            dma((n_sp,)),
            dma((n_sp,)),
            dma,
            dma,
            dma((n_tp,)),
            dma((n_tp,)),
            dma((n_tp,)),
            dma((n_tp,)),
        ],
        compiler_params=pltpu.CompilerParams(
            collective_id=0, has_side_effects=True, vmem_limit_bytes=VMEM_LIMIT
        ),
        name="layer",
    )(
        tokens,
        w_query,
        w_key,
        w_value,
        w_gate,
        w_pool,
        norm_gain.reshape(1, HEAD),
        log_decay.reshape(rows // HEAD, HEAD),
        w_out,
        fine,
        base,
    )
def solution(mesh):
    in_specs = (
        P("sp", None),
        P(None, "tp"),
        P(None, "tp"),
        P(None, "tp"),
        P(None, "tp"),
        P(None, "tp"),
        P("tp"),
        P("tp", "sp"),
        P(),
    )
    body = functools.partial(local, mesh.shape["sp"], mesh.shape["tp"])
    return jax.shard_map(
        body, mesh=mesh, in_specs=in_specs, out_specs=P(("sp", "tp"), None), check_vma=False
    )
```

```python
import functools

import jax
import jax.numpy as jnp
import numpy as np
from jax import lax
from jax.experimental import pallas as pl
from jax.experimental.pallas import tpu as pltpu
from jax.sharding import PartitionSpec as P

HEAD = 128
CHUNK = 256
HALO = 16
SIDE = 4
ROW_AT = 0
F32 = jnp.float32
BF16 = jnp.bfloat16
VMEM_LIMIT = 62 * 1024 * 1024 + 512 * 1024


def dot(a, b):
    return jnp.dot(a, b, preferred_element_type=F32)


def dot_nt(a, b):
    return lax.dot_general(a, b, (((1,), (1,)), ((), ())), preferred_element_type=F32)


def dot_tn(a, b):
    return lax.dot_general(a, b, (((0,), (0,)), ((), ())), preferred_element_type=F32)


def angle_tables(positions):
    half = HEAD // 2
    inverse = 10000.0 ** (-np.arange(half, dtype=np.float64) / half)
    angles = np.asarray(positions, np.float64)[:, None] * inverse[None, :]
    cosine, sine = np.cos(angles), np.sin(angles)
    return (
        np.concatenate([cosine, cosine], axis=1).astype(np.float32),
        np.concatenate([-sine, sine], axis=1).astype(np.float32),
    )


def lane_cumsum(x):
    lane = lax.broadcasted_iota(jnp.int32, x.shape, 1)
    step = 1
    while step < x.shape[1]:
        x = x + jnp.where(lane >= step, pltpu.roll(x, step, 1), 0.0)
        step *= 2
    return x


def kernel(
    n_sp,
    n_tp,
    tok_hbm,
    wq_hbm,
    wk_hbm,
    wv_hbm,
    wg_hbm,
    wp_hbm,
    gain_hbm,
    ld_hbm,
    wout_hbm,
    fine_hbm,
    base_hbm,
    obuf_ref,
    x_ref,
    wkv_ref,
    wqg_ref,
    wp_ref,
    wout_ref,
    gain_ref,
    ld_ref,
    fine_ref,
    base_ref,
    k_ref,
    v_ref,
    q_ref,
    g_ref,
    p_ref,
    halo_ref,
    halo_send,
    acc_ref,
    lc_ref,
    lct_ref,
    ecol_ref,
    d_ref,
    be_ref,
    pre_ref,
    sloc_ref,
    ssend_ref,
    srecv_ref,
    tsend_ref,
    trecv_ref,
    rsend_ref,
    rrecv_ref,
    usend_ref,
    urecv_ref,
    pref_ref,
    upto_ref,
    inc_ref,
    psend_ref,
    gsend_ref,
    prow_ref,
    grow_ref,
    oacc_ref,
    tok_sem,
    in_sem,
    wout_sem,
    tsend_sem,
    trecv_sem,
    ssend_sem,
    srecv_sem,
    rsend_sem,
    rrecv_sem,
    usend_sem,
    urecv_sem,
    hsend_sem,
    hrecv_sem,
    psend_sem,
    precv_sem,
    gsend_sem,
    grecv_sem,
):
    sp = lax.axis_index("sp")
    tp = lax.axis_index("tp")
    rows = x_ref.shape[0]
    n_ch = rows // CHUNK
    width = wout_ref.shape[0] // 2
    n_x = n_tp // 2

    barrier = pltpu.get_barrier_semaphore()
    n_y = SIDE
    n_z = n_sp // n_y
    z, y = lax.div(sp, n_y), lax.rem(sp, n_y)

    def row_peer(j):
        return z * n_y + lax.rem(y + j, n_y)

    def column_peer(j):
        return lax.rem(z + j, n_z) * n_y + y

    sp_peers = [row_peer(j) for j in range(1, n_y)]
    sp_peers += [column_peer(j) for j in range(1, n_z)]
    sp_peers += [lax.rem(sp + 1, n_sp), lax.rem(sp + n_sp - 1, n_sp)]
    for peer in sp_peers:
        pl.semaphore_signal(barrier, inc=1, device_id={"sp": peer})
    for j in range(1, n_tp):
        pl.semaphore_signal(barrier, inc=1, device_id={"tp": lax.rem(tp + j, n_tp)})

    small = [
        pltpu.make_async_copy(ld_hbm, ld_ref, in_sem.at[0]),
        pltpu.make_async_copy(fine_hbm, fine_ref, in_sem.at[1]),
        pltpu.make_async_copy(
            base_hbm.at[:, pl.ds(pl.multiple_of(sp * n_ch, n_ch), n_ch), :], base_ref, in_sem.at[2]
        ),
        pltpu.make_async_copy(gain_hbm, gain_ref, in_sem.at[3]),
    ]
    w_copies = [
        pltpu.make_async_copy(wk_hbm, wkv_ref.at[:, 0:HEAD], in_sem.at[4]),
        pltpu.make_async_copy(wv_hbm, wkv_ref.at[:, HEAD : 2 * HEAD], in_sem.at[5]),
        pltpu.make_async_copy(wp_hbm, wp_ref, in_sem.at[6]),
        pltpu.make_async_copy(wq_hbm, wqg_ref.at[:, 0:HEAD], in_sem.at[7]),
        pltpu.make_async_copy(wg_hbm, wqg_ref.at[:, HEAD : 2 * HEAD], in_sem.at[8]),
    ]

    def chunk_of(c):
        if isinstance(c, int):
            return slice(c * CHUNK, (c + 1) * CHUNK)
        return pl.ds(pl.multiple_of(c * CHUNK, CHUNK), CHUNK)

    def tok_copy(c):
        return pltpu.make_async_copy(
            tok_hbm.at[chunk_of(c), :], x_ref.at[chunk_of(c), :], tok_sem.at[c]
        )

    wout_copy = pltpu.make_async_copy(wout_hbm, wout_ref, wout_sem)

    for copy in small[:3]:
        copy.start()
    w_copies[0].start()
    w_copies[1].start()
    tok_copy(0).start()
    tok_copy(1).start()

    small[0].wait()
    tok_copy(2).start()
    tok_copy(3).start()
    lc = lane_cumsum(ld_ref[...])
    lc_ref[...] = lc
    lct_ref[...] = jnp.transpose(lc)
    run = jnp.zeros((1, 1), F32)
    for c in range(n_ch):
        end = lc[2 * c : 2 * c + 1, HEAD - 1 :] + lc[2 * c + 1 : 2 * c + 2, HEAD - 1 :]
        be_ref[c : c + 1, :] = jnp.broadcast_to(jnp.exp(end), (1, HEAD))
        pre_ref[c : c + 1, :] = jnp.broadcast_to(jnp.exp(run), (1, HEAD))
        run = run + end
    tsend_ref[...] = jnp.broadcast_to(run, tsend_ref.shape)

    def columns(c):
        first = jnp.broadcast_to(lct_ref[:, 2 * c : 2 * c + 1], (HEAD, HEAD))
        second = jnp.broadcast_to(lct_ref[:, 2 * c + 1 : 2 * c + 2], (HEAD, HEAD))
        return first, second + lc_ref[2 * c : 2 * c + 1, HEAD - 1 :]

    def decay_of_chunk(c):
        row_a = lc_ref[2 * c : 2 * c + 1, :]
        row_b = lc_ref[2 * c + 1 : 2 * c + 2, :] + row_a[:, HEAD - 1 :]
        col_a, col_b = columns(c)
        low = lax.broadcasted_iota(jnp.int32, (HEAD, HEAD), 0) >= lax.broadcasted_iota(
            jnp.int32, (HEAD, HEAD), 1
        )
        d_ref[c, :HEAD, :HEAD] = jnp.where(low, jnp.exp(jnp.minimum(col_a - row_a, 0.0)), 0.0)
        d_ref[c, :HEAD, HEAD:] = jnp.zeros((HEAD, HEAD), F32)
        d_ref[c, HEAD:, :HEAD] = jnp.exp(col_b - row_a)
        d_ref[c, HEAD:, HEAD:] = jnp.where(low, jnp.exp(jnp.minimum(col_b - row_b, 0.0)), 0.0)
        ecol_ref[c * CHUNK : c * CHUNK + HEAD, :] = jnp.exp(col_a)
        ecol_ref[c * CHUNK + HEAD : (c + 1) * CHUNK, :] = jnp.exp(col_b)

    def pushed(src, dst, slot, peer, send_sem, recv_sem, at):
        return pltpu.make_async_remote_copy(
            src_ref=src,
            dst_ref=dst.at[slot],
            send_sem=send_sem.at[at],
            recv_sem=recv_sem.at[slot],
            device_id={"sp": peer},
            device_id_type=pl.DeviceIdType.MESH,
        )

    def row_sends(j):
        return (
            pushed(tsend_ref, trecv_ref, y, row_peer(j), tsend_sem, trecv_sem, j),
            pushed(ssend_ref, srecv_ref, y, row_peer(j), ssend_sem, srecv_sem, j),
        )

    def column_sends(j):
        return (
            pushed(usend_ref, urecv_ref, z, column_peer(j), usend_sem, urecv_sem, j),
            pushed(rsend_ref, rrecv_ref, z, column_peer(j), rsend_sem, rrecv_sem, j),
        )

    small[1].wait()
    small[2].wait()
    w_copies[0].wait()
    w_copies[1].wait()

    def turned(x, c):
        base_c = base_ref[0, pl.ds(c, 1), :]
        base_s = base_ref[1, pl.ds(c, 1), :]
        fine_c = fine_ref[0]
        fine_s = fine_ref[1]
        cosine = base_c * fine_c - base_s * fine_s
        sine = base_s * fine_c + base_c * fine_s
        return x * cosine + pltpu.roll(x, HEAD // 2, 1) * sine

    def kv_of(c):
        if c == 0:
            tok_copy(0).wait()
            tok_copy(1).wait()
            for later in range(4, n_ch):
                tok_copy(later).start()
            w_copies[2].start()
        if c == 2:
            tok_copy(2).wait()
            tok_copy(3).wait()
        if c == 4:
            for later in range(4, n_ch):
                tok_copy(later).wait()
            for copy in w_copies[3:]:
                copy.start()
            small[3].start()
        return dot(x_ref[chunk_of(c), :], wkv_ref[...])

    def keep_kv(c, kv, state):
        here = chunk_of(c)
        key = kv[:, :HEAD].astype(BF16).astype(F32)
        value = kv[:, HEAD:].astype(BF16)
        k_rot = (turned(key, c) * HEAD**-0.5).astype(BF16)
        k_ref[here, :] = k_rot
        v_ref[here, :] = value
        col_a, col_b = columns(c)
        end = col_b[HEAD - 1 :, :]
        fade = jnp.concatenate([jnp.exp(end - col_a), jnp.exp(end - col_b)], axis=0)
        decayed = (k_rot.astype(F32) * fade).astype(BF16)
        update = dot_tn(decayed, value)
        sloc_ref[c] = state.astype(BF16)
        return state * be_ref[pl.ds(c, 1), :] + update

    state = jnp.zeros((HEAD, HEAD), F32)
    kv = kv_of(0)
    for c in range(n_ch):
        if c + 1 < n_ch:
            kv_next = kv_of(c + 1)
        state = keep_kv(c, kv, state)
        kv = kv_next
    wout_copy.start()
    w_copies[2].wait()
    halo_send[...] = dot(x_ref[rows - HALO :, :], wp_ref[...]).astype(BF16)
    ssend_ref[...] = state.astype(BF16)
    srecv_ref[y] = state.astype(BF16)
    trecv_ref[y] = tsend_ref[...]

    pl.semaphore_wait(barrier, len(sp_peers) + n_tp - 1)
    halo_copy = pltpu.make_async_remote_copy(
        src_ref=halo_send,
        dst_ref=halo_ref,
        send_sem=hsend_sem,
        recv_sem=hrecv_sem,
        device_id={"sp": lax.rem(sp + 1, n_sp)},
        device_id_type=pl.DeviceIdType.MESH,
    )

    @pl.when(sp + 1 < n_sp)
    def _():
        halo_copy.start()

    for j in (2, 1, 3):
        for copy in row_sends(j):
            copy.start()

    x_at, core = lax.div(tp, 2), lax.rem(tp, 2)
    order = [(2, 0), (3, 0), (2, 1), (3, 1), (1, 0), (1, 1), (0, 1), (0, 0)]

    def peer_of(dx, dc):
        return lax.rem(x_at + dx, n_x) * 2 + lax.rem(core + dc, 2)

    def row_copy(peer, send_ref, recv_ref, send_sem, recv_sem):
        return pltpu.make_async_remote_copy(
            src_ref=send_ref.at[peer],
            dst_ref=recv_ref.at[tp],
            send_sem=send_sem.at[peer],
            recv_sem=recv_sem.at[tp],
            device_id={"tp": peer},
            device_id_type=pl.DeviceIdType.MESH,
        )

    def recv_wait(j, send_ref, recv_ref, send_sem, recv_sem):
        pltpu.make_async_remote_copy(
            src_ref=send_ref.at[0],
            dst_ref=recv_ref.at[j],
            send_sem=send_sem.at[0],
            recv_sem=recv_sem.at[j],
            device_id={"tp": tp},
            device_id_type=pl.DeviceIdType.MESH,
        ).wait_recv()

    group = lax.div(tp * HEAD, 256)
    window = jnp.left_shift(jnp.int32(2), group)

    def pooled_of(c):
        x = p_ref[c * CHUNK : (c + 1) * CHUNK + HALO, :]
        s = x + pltpu.roll(x, 1, 0)
        for level in (1, 2, 3):
            s = jnp.where(group >= level, s + pltpu.roll(s, 2**level, 0), s)
        s = s[HALO:, :]
        x = x[HALO:, :]
        at = lax.broadcasted_iota(jnp.int32, (HALO, HEAD), 0) + (sp * rows + c * CHUNK + 1)
        count = jnp.minimum(at, window).astype(F32)
        whole = jnp.minimum(lax.broadcasted_iota(jnp.int32, (1, HEAD), 1) + 4096, window).astype(F32)
        top = s[:HALO, :] / count
        rest = s[HALO:, :] * (1.0 / whole)
        return (jnp.concatenate([top, rest], axis=0) - x).astype(BF16)

    p_args = (psend_ref, prow_ref, psend_sem, precv_sem)
    g_args = (gsend_ref, grow_ref, gsend_sem, grecv_sem)

    def p_of(c):
        return dot(x_ref[chunk_of(c), :], wp_ref[...])

    p = p_of(0)
    for c in range(n_ch):
        if c + 1 < n_ch:
            p_next = p_of(c + 1)
        p_ref[HALO + c * CHUNK : HALO + (c + 1) * CHUNK, :] = p.astype(BF16).astype(F32)
        decay_of_chunk(c)
        if c > 0:
            psend_ref[c] = pooled_of(c)
        p = p_next

    @pl.when(sp > 0)
    def _():
        halo_copy.wait_recv()
        p_ref[0:HALO, :] = halo_ref[...].astype(F32)

    @pl.when(sp == 0)
    def _():
        p_ref[0:HALO, :] = jnp.zeros((HALO, HEAD), F32)

    psend_ref[0] = pooled_of(0)
    for k in range(n_tp - 1):
        row_copy(peer_of(*order[k]), *p_args).start()
    prow_ref[tp] = psend_ref[tp]

    w_copies[3].wait()
    w_copies[4].wait()
    def keep_q(c, qg):
        here = chunk_of(c)
        query = qg[:, :HEAD].astype(BF16).astype(F32)
        g_ref[here, :] = qg[:, HEAD:].astype(BF16)
        q_rot = turned(query, c).astype(BF16)
        q_ref[here, :] = q_rot
        scores = dot_nt(q_rot, k_ref[here, :])
        mixing = (scores * d_ref[c]).astype(BF16)
        inner = dot(mixing, v_ref[here, :])
        cross = dot(q_rot, sloc_ref[c]) * ecol_ref[here, :]
        acc_ref[here, :] = inner + cross

    def row_states():
        for j in range(1, n_y):
            slot = lax.rem(y + j, n_y)
            pushed(tsend_ref, trecv_ref, slot, sp, tsend_sem, trecv_sem, 0).wait_recv()
            pushed(ssend_ref, srecv_ref, slot, sp, ssend_sem, srecv_sem, 0).wait_recv()
        total = jnp.zeros((HEAD, HEAD), F32)
        before = jnp.zeros((HEAD, HEAD), F32)
        reach = jnp.zeros((1, HEAD), F32)
        upto = jnp.zeros((1, HEAD), F32)
        for j in range(n_y):
            before = jnp.where(y == j, total, before)
            upto = jnp.where(y == j, reach, upto)
            decay = trecv_ref[j, 0:1, :]
            total = total * jnp.exp(decay) + srecv_ref[j].astype(F32)
            reach = reach + decay
        pref_ref[...] = before
        upto_ref[...] = jnp.broadcast_to(jnp.exp(upto), upto_ref.shape)
        usend_ref[...] = jnp.broadcast_to(reach, usend_ref.shape)
        rsend_ref[...] = total.astype(BF16)
        for j in range(1, n_z):

            @pl.when(z + j < n_z)
            def _():
                for copy in column_sends(j):
                    copy.start()

    qg = dot(x_ref[chunk_of(0), :], wqg_ref[...])
    for c in range(n_ch):
        if c + 1 < n_ch:
            qg_next = dot(x_ref[chunk_of(c + 1), :], wqg_ref[...])
        keep_q(c, qg)
        qg = qg_next
        if c == ROW_AT:
            row_states()

    inc_ref[...] = jnp.zeros_like(inc_ref)

    def inc_step(j, carry):
        pushed(usend_ref, urecv_ref, j, sp, usend_sem, urecv_sem, 0).wait_recv()
        pushed(rsend_ref, rrecv_ref, j, sp, rsend_sem, rrecv_sem, 0).wait_recv()
        inc_ref[...] = inc_ref[...] * jnp.exp(urecv_ref[j, 0:1, :]) + rrecv_ref[j].astype(F32)
        return carry

    lax.fori_loop(0, z, inc_step, 0)
    incoming = (inc_ref[...] * upto_ref[0:1, :] + pref_ref[...]).astype(BF16)

    small[3].wait()

    def gated_of(c):
        here = chunk_of(c)
        cross = dot(q_ref[here, :], incoming) * (ecol_ref[here, :] * pre_ref[pl.ds(c, 1), :])
        retained = acc_ref[here, :] + cross
        centered = retained - jnp.mean(retained, axis=-1, keepdims=True)
        scale = lax.rsqrt(jnp.mean(centered * centered, axis=-1, keepdims=True) + 1e-06)
        gate = g_ref[here, :].astype(F32)
        return (gate * jax.nn.sigmoid(gate) * gain_ref[...] * (centered * scale)).astype(BF16)

    for k in range(n_tp - 1):
        peer = peer_of(*order[k])
        gsend_ref[peer] = gated_of(peer)
        row_copy(peer, *g_args).start()
    grow_ref[tp] = gated_of(tp)

    wout_copy.wait()
    for j in range(n_tp):

        @pl.when(tp != j)
        def _():
            recv_wait(j, *p_args)

    n_cols = wout_ref.shape[1]
    tile = 256
    pool_rows = jnp.concatenate([prow_ref[j] for j in range(n_tp)], axis=1)

    tiles = [slice(i * tile, (i + 1) * tile) for i in range(n_cols // tile)]
    for at in tiles:
        oacc_ref[:, at] = dot(pool_rows, wout_ref[width:, at])

    for n, dx in enumerate((0, 2, 1, 3)):
        pair = lax.rem(x_at + dx, n_x)
        if dx == 0:
            recv_wait(pair * 2 + 1 - core, *g_args)
        else:
            recv_wait(pair * 2, *g_args)
            recv_wait(pair * 2 + 1, *g_args)
        lhs = jnp.concatenate([grow_ref[pair * 2], grow_ref[pair * 2 + 1]], axis=1)
        deep = pl.ds(pl.multiple_of(pair * 2 * HEAD, 2 * HEAD), 2 * HEAD)

        for at in tiles:
            total = oacc_ref[:, at] + dot(lhs, wout_ref[deep, at])
            if n < 3:
                oacc_ref[:, at] = total
            else:
                obuf_ref[:, at] = total.astype(BF16)

    for j in range(1, n_y):
        for copy in row_sends(j):
            copy.wait_send()
    for j in range(1, n_z):

        @pl.when(z + j < n_z)
        def _():
            for copy in column_sends(j):
                copy.wait_send()

    @pl.when(sp + 1 < n_sp)
    def _():
        halo_copy.wait_send()

    for k in range(n_tp - 1):
        peer = peer_of(*order[k])
        row_copy(peer, *p_args).wait_send()
        row_copy(peer, *g_args).wait_send()


def local(n_sp, n_tp, tokens, w_query, w_key, w_value, w_gate, w_pool, norm_gain, log_decay, w_out):
    rows, depth = tokens.shape
    n_ch = rows // CHUNK
    out_rows, out_cols = rows // n_tp, w_out.shape[1]
    fine = np.stack(angle_tables(np.arange(CHUNK)))
    base = np.stack(angle_tables(np.arange(n_sp * n_ch) * CHUNK))
    any_spec = pl.BlockSpec(memory_space=pltpu.HBM)
    dma = pltpu.SemaphoreType.DMA
    vm = pltpu.VMEM
    return pl.pallas_call(
        functools.partial(kernel, n_sp, n_tp),
        out_shape=pltpu.VMEM((out_rows, out_cols), BF16),
        in_specs=[any_spec] * 11,
        out_specs=pl.BlockSpec(memory_space=pltpu.VMEM),
        scratch_shapes=[
            vm((rows, depth), BF16),
            vm((depth, 2 * HEAD), BF16),
            vm((depth, 2 * HEAD), BF16),
            vm((depth, HEAD), BF16),
            vm(w_out.shape, BF16),
            vm((1, HEAD), F32),
            vm((rows // HEAD, HEAD), F32),
            vm((2, CHUNK, HEAD), F32),
            vm((2, n_ch, HEAD), F32),
            vm((rows, HEAD), BF16),
            vm((rows, HEAD), BF16),
            vm((rows, HEAD), BF16),
            vm((rows, HEAD), BF16),
            vm((rows + HALO, HEAD), F32),
            vm((HALO, HEAD), BF16),
            vm((HALO, HEAD), BF16),
            vm((rows, HEAD), F32),
            vm((rows // HEAD, HEAD), F32),
            vm((HEAD, rows // HEAD), F32),
            vm((rows, HEAD), F32),
            vm((n_ch, CHUNK, CHUNK), F32),
            vm((n_ch, HEAD), F32),
            vm((n_ch, HEAD), F32),
            vm((n_ch, HEAD, HEAD), BF16),
            vm((HEAD, HEAD), BF16),
            vm((SIDE, HEAD, HEAD), BF16),
            vm((8, HEAD), F32),
            vm((SIDE, 8, HEAD), F32),
            vm((HEAD, HEAD), BF16),
            vm((n_sp // SIDE, HEAD, HEAD), BF16),
            vm((8, HEAD), F32),
            vm((n_sp // SIDE, 8, HEAD), F32),
            vm((HEAD, HEAD), F32),
            vm((8, HEAD), F32),
            vm((HEAD, HEAD), F32),
            vm((n_tp, CHUNK, HEAD), BF16),
            vm((n_tp, CHUNK, HEAD), BF16),
            vm((n_tp, CHUNK, HEAD), BF16),
            vm((n_tp, CHUNK, HEAD), BF16),
            vm((out_rows, out_cols), F32),
            dma((n_ch,)),
            dma((9,)),
            dma,
            dma((SIDE,)),
            dma((SIDE,)),
            dma((SIDE,)),
            dma((SIDE,)),
            dma((n_sp // SIDE,)),
            dma((n_sp // SIDE,)),
            dma((n_sp // SIDE,)),
            dma((n_sp // SIDE,)),
            dma,
            dma,
            dma((n_tp,)),
            dma((n_tp,)),
            dma((n_tp,)),
            dma((n_tp,)),
        ],
        compiler_params=pltpu.CompilerParams(
            collective_id=0, has_side_effects=True, vmem_limit_bytes=VMEM_LIMIT
        ),
        name="layer",
    )(
        tokens,
        w_query,
        w_key,
        w_value,
        w_gate,
        w_pool,
        norm_gain.reshape(1, HEAD),
        log_decay.reshape(rows // HEAD, HEAD),
        w_out,
        fine,
        base,
    )
def solution(mesh):
    in_specs = (
        P("sp", None),
        P(None, "tp"),
        P(None, "tp"),
        P(None, "tp"),
        P(None, "tp"),
        P(None, "tp"),
        P("tp"),
        P("tp", "sp"),
        P(),
    )
    body = functools.partial(local, mesh.shape["sp"], mesh.shape["tp"])
    return jax.shard_map(
        body, mesh=mesh, in_specs=in_specs, out_specs=P(("sp", "tp"), None), check_vma=False
    )
```

```python
import functools

import jax
import jax.numpy as jnp
import numpy as np
from jax import lax
from jax.experimental import pallas as pl
from jax.experimental.pallas import tpu as pltpu
from jax.sharding import PartitionSpec as P

HEAD = 128
CHUNK = 256
HALO = 16
SIDE = 4
PAD = 8
EARLY = 4
LOG_SCALE = -0.5 * float(np.log(HEAD))
ROW_AT = 3
HALO_AT = 2
F32 = jnp.float32
BF16 = jnp.bfloat16
VMEM_LIMIT = 62 * 1024 * 1024 + 512 * 1024


def dot(a, b):
    return jnp.dot(a, b, preferred_element_type=F32)


def dot_nt(a, b):
    return lax.dot_general(a, b, (((1,), (1,)), ((), ())), preferred_element_type=F32)


def dot_tn(a, b):
    return lax.dot_general(a, b, (((0,), (0,)), ((), ())), preferred_element_type=F32)


def angle_tables(positions):
    half = HEAD // 2
    inverse = 10000.0 ** (-np.arange(half, dtype=np.float64) / half)
    angles = np.asarray(positions, np.float64)[:, None] * inverse[None, :]
    cosine, sine = np.cos(angles), np.sin(angles)
    return (
        np.concatenate([cosine, cosine], axis=1).astype(np.float32),
        np.concatenate([-sine, sine], axis=1).astype(np.float32),
    )


def lane_cumsum(x):
    lane = lax.broadcasted_iota(jnp.int32, x.shape, 1)
    step = 1
    while step < x.shape[1]:
        x = x + jnp.where(lane >= step, pltpu.roll(x, step, 1), 0.0)
        step *= 2
    return x


def kernel(
    n_sp,
    n_tp,
    tok_hbm,
    wq_hbm,
    wk_hbm,
    wv_hbm,
    wg_hbm,
    wp_hbm,
    gain_hbm,
    ld_hbm,
    wout_hbm,
    fine_hbm,
    base_hbm,
    obuf_ref,
    x_ref,
    wkv_ref,
    wqg_ref,
    wp_ref,
    wout_ref,
    gain_ref,
    ld_ref,
    fine_ref,
    base_ref,
    k_ref,
    v_ref,
    faded_ref,
    q_ref,
    g_ref,
    p_ref,
    halo_ref,
    halo_send,
    acc_ref,
    lc_ref,
    lct_ref,
    cos_ref,
    sin_ref,
    fade_ref,
    shift_ref,
    ecol_ref,
    edev_ref,
    d_ref,
    be_ref,
    pre_ref,
    sloc_ref,
    ssend_ref,
    srecv_ref,
    tsend_ref,
    trecv_ref,
    rsend_ref,
    rrecv_ref,
    usend_ref,
    urecv_ref,
    pref_ref,
    upto_ref,
    inc_ref,
    psend_ref,
    gsend_ref,
    prow_ref,
    grow_ref,
    oacc_ref,
    tok_sem,
    in_sem,
    wout_sem,
    tsend_sem,
    trecv_sem,
    ssend_sem,
    srecv_sem,
    rsend_sem,
    rrecv_sem,
    usend_sem,
    urecv_sem,
    hsend_sem,
    hrecv_sem,
    psend_sem,
    precv_sem,
    gsend_sem,
    grecv_sem,
):
    sp = lax.axis_index("sp")
    tp = lax.axis_index("tp")
    rows = x_ref.shape[0] - HALO
    n_ch = rows // CHUNK
    width = wout_ref.shape[0] // 2
    n_x = n_tp // 2

    barrier = pltpu.get_barrier_semaphore()
    n_y = SIDE
    n_z = n_sp // n_y
    z, y = lax.div(sp, n_y), lax.rem(sp, n_y)

    def row_peer(j):
        return z * n_y + lax.rem(y + j, n_y)

    def column_peer(j):
        return lax.rem(z + j, n_z) * n_y + y

    sp_peers = [row_peer(j) for j in range(1, n_y)]
    sp_peers += [column_peer(j) for j in range(1, n_z)]
    for peer in sp_peers:
        pl.semaphore_signal(barrier, inc=1, device_id={"sp": peer})

    @pl.when(sp + 1 < n_sp)
    def _():
        pl.semaphore_signal(barrier, inc=1, device_id={"sp": lax.rem(sp + 1, n_sp)})

    @pl.when(sp > 0)
    def _():
        pl.semaphore_signal(barrier, inc=1, device_id={"sp": lax.rem(sp + n_sp - 1, n_sp)})

    met = len(sp_peers) + n_tp - 1 + jnp.minimum(sp, 1) + jnp.minimum(n_sp - 1 - sp, 1)
    for j in range(1, n_tp):
        pl.semaphore_signal(barrier, inc=1, device_id={"tp": lax.rem(tp + j, n_tp)})

    small = [
        pltpu.make_async_copy(ld_hbm, ld_ref, in_sem.at[0]),
        pltpu.make_async_copy(fine_hbm, fine_ref, in_sem.at[1]),
        pltpu.make_async_copy(
            base_hbm.at[:, pl.ds(pl.multiple_of(sp * n_ch, n_ch), n_ch), :], base_ref, in_sem.at[2]
        ),
        pltpu.make_async_copy(gain_hbm, gain_ref, in_sem.at[3]),
    ]
    w_copies = [
        pltpu.make_async_copy(wk_hbm, wkv_ref.at[:, 0:HEAD], in_sem.at[4]),
        pltpu.make_async_copy(wv_hbm, wkv_ref.at[:, HEAD : 2 * HEAD], in_sem.at[5]),
        pltpu.make_async_copy(wp_hbm, wp_ref, in_sem.at[6]),
        pltpu.make_async_copy(wq_hbm, wqg_ref.at[:, 0:HEAD], in_sem.at[7]),
        pltpu.make_async_copy(wg_hbm, wqg_ref.at[:, HEAD : 2 * HEAD], in_sem.at[8]),
    ]

    def chunk_of(c):
        if isinstance(c, int):
            return slice(c * CHUNK, (c + 1) * CHUNK)
        return pl.ds(pl.multiple_of(c * CHUNK, CHUNK), CHUNK)

    def x_rows(c):
        return slice(HALO + c * CHUNK, HALO + (c + 1) * CHUNK)

    def tok_copy(c):
        return pltpu.make_async_copy(
            tok_hbm.at[chunk_of(c), :], x_ref.at[x_rows(c), :], tok_sem.at[c]
        )

    wout_copy = pltpu.make_async_copy(wout_hbm, wout_ref, wout_sem)

    for copy in small[:3]:
        copy.start()
    w_copies[0].start()
    w_copies[1].start()
    tok_copy(0).start()
    tok_copy(1).start()

    small[0].wait()
    w_copies[2].start()
    tok_copy(2).start()
    tok_copy(3).start()
    lc = lane_cumsum(ld_ref[...])
    lc_ref[...] = lc
    lct_ref[...] = jnp.transpose(lc)
    run = jnp.zeros((1, 1), F32)
    for c in range(n_ch):
        end = lc[2 * c : 2 * c + 1, HEAD - 1 :] + lc[2 * c + 1 : 2 * c + 2, HEAD - 1 :]
        be_ref[c : c + 1, :] = jnp.broadcast_to(jnp.exp(end), (1, HEAD))
        pre_ref[c : c + 1, :] = jnp.broadcast_to(jnp.exp(run), (1, HEAD))
        run = run + end
    tsend_ref[...] = jnp.broadcast_to(run, tsend_ref.shape)

    def columns(c):
        first = jnp.broadcast_to(lct_ref[:, 2 * c : 2 * c + 1], (HEAD, HEAD))
        second = jnp.broadcast_to(lct_ref[:, 2 * c + 1 : 2 * c + 2], (HEAD, HEAD))
        return first, second + lc_ref[2 * c : 2 * c + 1, HEAD - 1 :]

    def decay_of_chunk(c):
        row_a = lc_ref[2 * c : 2 * c + 1, :]
        row_b = lc_ref[2 * c + 1 : 2 * c + 2, :] + row_a[:, HEAD - 1 :]
        col_a, col_b = columns(c)
        low = lax.broadcasted_iota(jnp.int32, (HEAD, HEAD), 0) >= lax.broadcasted_iota(
            jnp.int32, (HEAD, HEAD), 1
        )
        sc_a, sc_b = col_a + LOG_SCALE, col_b + LOG_SCALE
        d_ref[c, :HEAD, :HEAD] = jnp.where(low, jnp.exp(sc_a - row_a), 0.0)
        d_ref[c, :HEAD, HEAD:] = jnp.zeros((HEAD, HEAD), F32)
        d_ref[c, HEAD:, :HEAD] = jnp.exp(sc_b - row_a)
        d_ref[c, HEAD:, HEAD:] = jnp.where(low, jnp.exp(sc_b - row_b), 0.0)
        here = chunk_of(c)
        within = jnp.exp(jnp.concatenate([col_a, col_b], axis=0))
        ecol_ref[here, :] = within
        edev_ref[here, :] = within * pre_ref[c : c + 1, :]

    def pushed(src, dst, slot, peer, send_sem, recv_sem, at):
        return pltpu.make_async_remote_copy(
            src_ref=src,
            dst_ref=dst.at[slot],
            send_sem=send_sem.at[at],
            recv_sem=recv_sem.at[slot],
            device_id={"sp": peer},
            device_id_type=pl.DeviceIdType.MESH,
        )

    def row_sends(j):
        return (
            pushed(tsend_ref, trecv_ref, y, row_peer(j), tsend_sem, trecv_sem, j),
            pushed(ssend_ref, srecv_ref, y, row_peer(j), ssend_sem, srecv_sem, j),
        )

    def column_sends(j):
        return (
            pushed(usend_ref, urecv_ref, z, column_peer(j), usend_sem, urecv_sem, j),
            pushed(rsend_ref, rrecv_ref, z, column_peer(j), rsend_sem, rrecv_sem, j),
        )

    small[1].wait()
    small[2].wait()
    for c in range(n_ch):
        here = chunk_of(c)
        base_c = base_ref[0, c : c + 1, :]
        base_s = base_ref[1, c : c + 1, :]
        fine_c = fine_ref[0]
        fine_s = fine_ref[1]
        cos_ref[here, :] = base_c * fine_c - base_s * fine_s
        sin_ref[here, :] = base_s * fine_c + base_c * fine_s
        col_a, col_b = columns(c)
        end = col_b[HEAD - 1 :, :] + LOG_SCALE
        fade_ref[here, :] = jnp.exp(jnp.concatenate([end - col_a, end - col_b], axis=0))
    p_ref[0 : PAD + HALO, :] = jnp.zeros((PAD + HALO, HEAD), F32)
    shift_ref[0:PAD, :] = jnp.zeros((PAD, HEAD), F32)
    for later in range(4, n_ch):
        tok_copy(later).start()
    w_copies[0].wait()
    w_copies[1].wait()
    w_copies[2].wait()

    def turned(x, c):
        here = chunk_of(c)
        return x * cos_ref[here, :] + pltpu.roll(x, HEAD // 2, 1) * sin_ref[here, :]

    x_at, core = lax.div(tp, 2), lax.rem(tp, 2)
    order = [(1, 0), (3, 0), (2, 0), (2, 1), (1, 1), (3, 1), (0, 1), (0, 0)]

    def peer_of(dx, dc):
        return lax.rem(x_at + dx, n_x) * 2 + lax.rem(core + dc, 2)

    def row_copy(peer, send_ref, recv_ref, send_sem, recv_sem):
        return pltpu.make_async_remote_copy(
            src_ref=send_ref.at[peer],
            dst_ref=recv_ref.at[tp],
            send_sem=send_sem.at[peer],
            recv_sem=recv_sem.at[tp],
            device_id={"tp": peer},
            device_id_type=pl.DeviceIdType.MESH,
        )

    def recv_wait(j, send_ref, recv_ref, send_sem, recv_sem):
        pltpu.make_async_remote_copy(
            src_ref=send_ref.at[0],
            dst_ref=recv_ref.at[j],
            send_sem=send_sem.at[0],
            recv_sem=recv_sem.at[j],
            device_id={"tp": tp},
            device_id_type=pl.DeviceIdType.MESH,
        ).wait_recv()

    group = lax.div(tp * HEAD, 256)
    window = jnp.left_shift(jnp.int32(2), group)

    def pooled_of(c):
        deep = CHUNK + HALO
        at = PAD + c * CHUNK
        x = p_ref[at : at + deep, :]
        s = x + p_ref[at - 1 : at - 1 + deep, :]
        for level in (1, 2, 3):
            shift_ref[PAD : PAD + deep, :] = s
            back = shift_ref[PAD - 2**level : PAD - 2**level + deep, :]
            s = jnp.where(group >= level, s + back, s)
        s = s[HALO:, :]
        x = x[HALO:, :]
        at = lax.broadcasted_iota(jnp.int32, (HALO, HEAD), 0) + (sp * rows + c * CHUNK + 1)
        count = jnp.minimum(at, window).astype(F32)
        whole = jnp.minimum(lax.broadcasted_iota(jnp.int32, (1, HEAD), 1) + 4096, window).astype(F32)
        top = s[:HALO, :] / count
        rest = s[HALO:, :] * (1.0 / whole)
        return (jnp.concatenate([top, rest], axis=0) - x).astype(BF16)

    p_args = (psend_ref, prow_ref, psend_sem, precv_sem)
    g_args = (gsend_ref, grow_ref, gsend_sem, grecv_sem)

    def p_of(c):
        return dot(x_ref[x_rows(c), :], wp_ref[...])

    def keep_p(c, p):
        p_ref[PAD + HALO + c * CHUNK : PAD + HALO + (c + 1) * CHUNK, :] = p
        if c > 0:
            psend_ref[c] = pooled_of(c)

    def send_pooled(*chunks):
        for c in chunks:

            @pl.when(tp != c)
            def _():
                row_copy(c, *p_args).start()

    def first_chunk():
        @pl.when(sp > 0)
        def _():
            halo_copy.wait_recv()
            p_ref[PAD : PAD + HALO, :] = halo_ref[...].astype(F32)

        psend_ref[0] = pooled_of(0)
        send_pooled(0)
        prow_ref[tp] = psend_ref[tp]

    peers = [peer_of(dx, dc) for dx, dc in order]

    def kv_of(c):
        if c == 0:
            tok_copy(0).wait()
            tok_copy(1).wait()
        if c == 2:
            tok_copy(2).wait()
            tok_copy(3).wait()
        if c == 4:
            for later in range(4, n_ch):
                tok_copy(later).wait()
            for copy in w_copies[3:]:
                copy.start()
            small[3].start()
            pl.semaphore_wait(barrier, met)
            send_pooled(*range(1, 3))
        return dot(x_ref[x_rows(c), :], wkv_ref[...])

    def keep_kv(c, kv):
        here = chunk_of(c)
        k_rot = turned(kv[:, :HEAD], c)
        k_ref[here, :] = k_rot.astype(BF16)
        v_ref[here, :] = kv[:, HEAD:].astype(BF16)
        faded_ref[c] = jnp.transpose((k_rot * fade_ref[here, :]).astype(BF16))

    def advance(c, state):
        sloc_ref[c] = state.astype(BF16)
        return state * be_ref[c : c + 1, :] + dot(faded_ref[c], v_ref[chunk_of(c), :])

    state = jnp.zeros((HEAD, HEAD), F32)
    kv = kv_of(0)
    for c in range(n_ch):
        if c + 1 < n_ch:
            kv_next = kv_of(c + 1)
        if c > 0:
            state = advance(c - 1, state)
        if c < EARLY:
            p = p_of(c)
        keep_kv(c, kv)
        if c < EARLY:
            keep_p(c, p)
        kv = kv_next
    state = advance(n_ch - 1, state)
    wout_copy.start()
    halo_send[...] = dot(x_ref[rows:, :], wp_ref[...]).astype(BF16)
    ssend_ref[...] = state.astype(BF16)
    srecv_ref[y] = state.astype(BF16)
    trecv_ref[y] = tsend_ref[...]

    halo_copy = pltpu.make_async_remote_copy(
        src_ref=halo_send,
        dst_ref=halo_ref,
        send_sem=hsend_sem,
        recv_sem=hrecv_sem,
        device_id={"sp": lax.rem(sp + 1, n_sp)},
        device_id_type=pl.DeviceIdType.MESH,
    )

    @pl.when(sp + 1 < n_sp)
    def _():
        halo_copy.start()

    for j in (2, 1, 3):
        for copy in row_sends(j):
            copy.start()

    p = p_of(EARLY)
    for c in range(EARLY, n_ch):
        if c + 1 < n_ch:
            p_next = p_of(c + 1)
        keep_p(c, p)
        for d in range(2 * (c - EARLY), min(n_ch, 2 * (c - EARLY) + 2)):
            decay_of_chunk(d)
        if c == EARLY + 1:
            send_pooled(*range(3, EARLY + 2))
        p = p_next
    send_pooled(*range(EARLY + 2, n_ch))

    w_copies[3].wait()
    w_copies[4].wait()
    def mix(c, qg):
        here = chunk_of(c)
        gate = qg[:, HEAD:]
        g_ref[here, :] = (gate * jax.nn.sigmoid(gate)).astype(BF16)
        q_rot = turned(qg[:, :HEAD], c).astype(BF16)
        q_ref[here, :] = q_rot
        return (dot_nt(q_rot, k_ref[here, :]) * d_ref[c]).astype(BF16)

    def retain(c, mixing):
        here = chunk_of(c)
        inner = dot(mixing, v_ref[here, :])
        acc_ref[here, :] = inner + dot(q_ref[here, :], sloc_ref[c]) * ecol_ref[here, :]

    def row_states():
        for j in range(1, n_y):
            slot = lax.rem(y + j, n_y)
            pushed(tsend_ref, trecv_ref, slot, sp, tsend_sem, trecv_sem, 0).wait_recv()
            pushed(ssend_ref, srecv_ref, slot, sp, ssend_sem, srecv_sem, 0).wait_recv()
        total = jnp.zeros((HEAD, HEAD), F32)
        before = jnp.zeros((HEAD, HEAD), F32)
        reach = jnp.zeros((1, HEAD), F32)
        upto = jnp.zeros((1, HEAD), F32)
        for j in range(n_y):
            before = jnp.where(y == j, total, before)
            upto = jnp.where(y == j, reach, upto)
            decay = trecv_ref[j, 0:1, :]
            total = total * jnp.exp(decay) + srecv_ref[j].astype(F32)
            reach = reach + decay
        pref_ref[...] = before
        upto_ref[...] = jnp.broadcast_to(jnp.exp(upto), upto_ref.shape)
        usend_ref[...] = jnp.broadcast_to(reach, usend_ref.shape)
        rsend_ref[...] = total.astype(BF16)
        for j in range(1, n_z):

            @pl.when(z + j < n_z)
            def _():
                for copy in column_sends(j):
                    copy.start()

    qg = dot(x_ref[x_rows(0), :], wqg_ref[...])
    mixing = None
    for c in range(n_ch):
        if c + 1 < n_ch:
            qg_next = dot(x_ref[x_rows(c + 1), :], wqg_ref[...])
        mixing_next = mix(c, qg)
        if c > 0:
            retain(c - 1, mixing)
        qg, mixing = qg_next, mixing_next
        if c == ROW_AT:
            row_states()
        if c == HALO_AT:
            first_chunk()
    retain(n_ch - 1, mixing)

    inc_ref[...] = jnp.zeros_like(inc_ref)

    def inc_step(j, carry):
        pushed(usend_ref, urecv_ref, j, sp, usend_sem, urecv_sem, 0).wait_recv()
        pushed(rsend_ref, rrecv_ref, j, sp, rsend_sem, rrecv_sem, 0).wait_recv()
        inc_ref[...] = inc_ref[...] * jnp.exp(urecv_ref[j, 0:1, :]) + rrecv_ref[j].astype(F32)
        return carry

    lax.fori_loop(0, z, inc_step, 0)
    incoming = (inc_ref[...] * upto_ref[0:1, :] + pref_ref[...]).astype(BF16)

    small[3].wait()

    def cross_of(c):
        return dot(q_ref[chunk_of(c), :], incoming)

    def gated_of(c, cross):
        here = chunk_of(c)
        retained = acc_ref[here, :] + cross * edev_ref[here, :]
        centered = retained - jnp.mean(retained, axis=-1, keepdims=True)
        scale = lax.rsqrt(jnp.mean(centered * centered, axis=-1, keepdims=True) + 1e-06)
        return (g_ref[here, :].astype(F32) * gain_ref[...] * (centered * scale)).astype(BF16)

    cross = cross_of(peers[0])
    for k, peer in enumerate(peers):
        if k + 1 < n_tp:
            cross_next = cross_of(peers[k + 1])
        chunk = gated_of(peer, cross)
        if k + 1 < n_tp:
            gsend_ref[peer] = chunk
            row_copy(peer, *g_args).start()
        else:
            grow_ref[tp] = chunk
        cross = cross_next

    wout_copy.wait()
    for j in range(n_tp):

        @pl.when(tp != j)
        def _():
            recv_wait(j, *p_args)

    n_cols = wout_ref.shape[1]
    tile = 256
    pool_rows = jnp.concatenate([prow_ref[j] for j in range(n_tp)], axis=1)

    tiles = [slice(i * tile, (i + 1) * tile) for i in range(n_cols // tile)]
    for at in tiles:
        oacc_ref[:, at] = dot(pool_rows, wout_ref[width:, at])

    for n, dx in enumerate((0, 2, 1, 3)):
        pair = lax.rem(x_at + dx, n_x)
        if dx == 0:
            recv_wait(pair * 2 + 1 - core, *g_args)
        else:
            recv_wait(pair * 2, *g_args)
            recv_wait(pair * 2 + 1, *g_args)
        lhs = jnp.concatenate([grow_ref[pair * 2], grow_ref[pair * 2 + 1]], axis=1)
        deep = pl.ds(pl.multiple_of(pair * 2 * HEAD, 2 * HEAD), 2 * HEAD)

        for at in tiles:
            total = oacc_ref[:, at] + dot(lhs, wout_ref[deep, at])
            if n < 3:
                oacc_ref[:, at] = total
            else:
                obuf_ref[:, at] = total.astype(BF16)

    for j in range(1, n_y):
        for copy in row_sends(j):
            copy.wait_send()
    for j in range(1, n_z):

        @pl.when(z + j < n_z)
        def _():
            for copy in column_sends(j):
                copy.wait_send()

    @pl.when(sp + 1 < n_sp)
    def _():
        halo_copy.wait_send()

    for k in range(n_tp - 1):
        peer = peer_of(*order[k])
        row_copy(peer, *p_args).wait_send()
        row_copy(peer, *g_args).wait_send()


def local(n_sp, n_tp, tokens, w_query, w_key, w_value, w_gate, w_pool, norm_gain, log_decay, w_out):
    rows, depth = tokens.shape
    n_ch = rows // CHUNK
    out_rows, out_cols = rows // n_tp, w_out.shape[1]
    fine = np.stack(angle_tables(np.arange(CHUNK)))
    base = np.stack(angle_tables(np.arange(n_sp * n_ch) * CHUNK))
    any_spec = pl.BlockSpec(memory_space=pltpu.HBM)
    dma = pltpu.SemaphoreType.DMA
    vm = pltpu.VMEM
    return pl.pallas_call(
        functools.partial(kernel, n_sp, n_tp),
        out_shape=pltpu.VMEM((out_rows, out_cols), BF16),
        in_specs=[any_spec] * 11,
        out_specs=pl.BlockSpec(memory_space=pltpu.VMEM),
        scratch_shapes=[
            vm((HALO + rows, depth), BF16),
            vm((depth, 2 * HEAD), BF16),
            vm((depth, 2 * HEAD), BF16),
            vm((depth, HEAD), BF16),
            vm(w_out.shape, BF16),
            vm((1, HEAD), F32),
            vm((rows // HEAD, HEAD), F32),
            vm((2, CHUNK, HEAD), F32),
            vm((2, n_ch, HEAD), F32),
            vm((rows, HEAD), BF16),
            vm((rows, HEAD), BF16),
            vm((n_ch, HEAD, CHUNK), BF16),
            vm((rows, HEAD), BF16),
            vm((rows, HEAD), BF16),
            vm((PAD + HALO + rows, HEAD), F32),
            vm((HALO, HEAD), BF16),
            vm((HALO, HEAD), BF16),
            vm((rows, HEAD), F32),
            vm((rows // HEAD, HEAD), F32),
            vm((HEAD, rows // HEAD), F32),
            vm((rows, HEAD), F32),
            vm((rows, HEAD), F32),
            vm((rows, HEAD), F32),
            vm((PAD + HALO + CHUNK, HEAD), F32),
            vm((rows, HEAD), F32),
            vm((rows, HEAD), F32),
            vm((n_ch, CHUNK, CHUNK), F32),
            vm((n_ch, HEAD), F32),
            vm((n_ch, HEAD), F32),
            vm((n_ch, HEAD, HEAD), BF16),
            vm((HEAD, HEAD), BF16),
            vm((SIDE, HEAD, HEAD), BF16),
            vm((8, HEAD), F32),
            vm((SIDE, 8, HEAD), F32),
            vm((HEAD, HEAD), BF16),
            vm((n_sp // SIDE, HEAD, HEAD), BF16),
            vm((8, HEAD), F32),
            vm((n_sp // SIDE, 8, HEAD), F32),
            vm((HEAD, HEAD), F32),
            vm((8, HEAD), F32),
            vm((HEAD, HEAD), F32),
            vm((n_tp, CHUNK, HEAD), BF16),
            vm((n_tp, CHUNK, HEAD), BF16),
            vm((n_tp, CHUNK, HEAD), BF16),
            vm((n_tp, CHUNK, HEAD), BF16),
            vm((out_rows, out_cols), F32),
            dma((n_ch,)),
            dma((9,)),
            dma,
            dma((SIDE,)),
            dma((SIDE,)),
            dma((SIDE,)),
            dma((SIDE,)),
            dma((n_sp // SIDE,)),
            dma((n_sp // SIDE,)),
            dma((n_sp // SIDE,)),
            dma((n_sp // SIDE,)),
            dma,
            dma,
            dma((n_tp,)),
            dma((n_tp,)),
            dma((n_tp,)),
            dma((n_tp,)),
        ],
        compiler_params=pltpu.CompilerParams(
            collective_id=0, has_side_effects=True, vmem_limit_bytes=VMEM_LIMIT
        ),
        name="layer",
    )(
        tokens,
        w_query,
        w_key,
        w_value,
        w_gate,
        w_pool,
        norm_gain.reshape(1, HEAD),
        log_decay.reshape(rows // HEAD, HEAD),
        w_out,
        fine,
        base,
    )
def solution(mesh):
    in_specs = (
        P("sp", None),
        P(None, "tp"),
        P(None, "tp"),
        P(None, "tp"),
        P(None, "tp"),
        P(None, "tp"),
        P("tp"),
        P("tp", "sp"),
        P(),
    )
    body = functools.partial(local, mesh.shape["sp"], mesh.shape["tp"])
    return jax.shard_map(
        body, mesh=mesh, in_specs=in_specs, out_specs=P(("sp", "tp"), None), check_vma=False
    )
```

```python
import functools

import jax
import jax.numpy as jnp
import numpy as np
from jax import lax
from jax.experimental import pallas as pl
from jax.experimental.pallas import tpu as pltpu
from jax.sharding import PartitionSpec as P

HEAD = 128
CHUNK = 256
HALO = 16
SIDE = 4
PAD = 8
EARLY = 4
LOG_SCALE = -0.5 * float(np.log(HEAD))
ROW_AT = 3
HALO_AT = 2
F32 = jnp.float32
BF16 = jnp.bfloat16
VMEM_LIMIT = 62 * 1024 * 1024 + 512 * 1024


def dot(a, b):
    return jnp.dot(a, b, preferred_element_type=F32)


def dot_nt(a, b):
    return lax.dot_general(a, b, (((1,), (1,)), ((), ())), preferred_element_type=F32)


def dot_tn(a, b):
    return lax.dot_general(a, b, (((0,), (0,)), ((), ())), preferred_element_type=F32)


def angle_tables(positions):
    half = HEAD // 2
    inverse = 10000.0 ** (-np.arange(half, dtype=np.float64) / half)
    angles = np.asarray(positions, np.float64)[:, None] * inverse[None, :]
    cosine, sine = np.cos(angles), np.sin(angles)
    return (
        np.concatenate([cosine, cosine], axis=1).astype(np.float32),
        np.concatenate([-sine, sine], axis=1).astype(np.float32),
    )


def lane_cumsum(x):
    lane = lax.broadcasted_iota(jnp.int32, x.shape, 1)
    step = 1
    while step < x.shape[1]:
        x = x + jnp.where(lane >= step, pltpu.roll(x, step, 1), 0.0)
        step *= 2
    return x


def kernel(
    n_sp,
    n_tp,
    tok_hbm,
    wq_hbm,
    wk_hbm,
    wv_hbm,
    wg_hbm,
    wp_hbm,
    gain_hbm,
    ld_hbm,
    wout_hbm,
    fine_hbm,
    base_hbm,
    obuf_ref,
    x_ref,
    wkv_ref,
    wqg_ref,
    wp_ref,
    wout_ref,
    gain_ref,
    ld_ref,
    fine_ref,
    base_ref,
    k_ref,
    v_ref,
    faded_ref,
    q_ref,
    g_ref,
    p_ref,
    halo_ref,
    halo_send,
    acc_ref,
    lc_ref,
    lct_ref,
    cos_ref,
    sin_ref,
    fade_ref,
    shift_ref,
    ecol_ref,
    edev_ref,
    d_ref,
    be_ref,
    pre_ref,
    sloc_ref,
    ssend_ref,
    srecv_ref,
    tsend_ref,
    trecv_ref,
    rsend_ref,
    rrecv_ref,
    usend_ref,
    urecv_ref,
    pref_ref,
    upto_ref,
    inc_ref,
    psend_ref,
    gsend_ref,
    prow_ref,
    grow_ref,
    oacc_ref,
    tok_sem,
    in_sem,
    wout_sem,
    tsend_sem,
    trecv_sem,
    ssend_sem,
    srecv_sem,
    rsend_sem,
    rrecv_sem,
    usend_sem,
    urecv_sem,
    hsend_sem,
    hrecv_sem,
    psend_sem,
    precv_sem,
    gsend_sem,
    grecv_sem,
):
    sp = lax.axis_index("sp")
    tp = lax.axis_index("tp")
    rows = x_ref.shape[0] - HALO
    n_ch = rows // CHUNK
    width = wout_ref.shape[0] // 2
    n_x = n_tp // 2

    barrier = pltpu.get_barrier_semaphore()
    n_y = SIDE
    n_z = n_sp // n_y
    z, y = lax.div(sp, n_y), lax.rem(sp, n_y)

    def row_peer(j):
        return z * n_y + lax.rem(y + j, n_y)

    def column_peer(j):
        return lax.rem(z + j, n_z) * n_y + y

    sp_peers = [row_peer(j) for j in range(1, n_y)]
    sp_peers += [column_peer(j) for j in range(1, n_z)]
    for peer in sp_peers:
        pl.semaphore_signal(barrier, inc=1, device_id={"sp": peer})

    @pl.when(sp + 1 < n_sp)
    def _():
        pl.semaphore_signal(barrier, inc=1, device_id={"sp": lax.rem(sp + 1, n_sp)})

    @pl.when(sp > 0)
    def _():
        pl.semaphore_signal(barrier, inc=1, device_id={"sp": lax.rem(sp + n_sp - 1, n_sp)})

    met = len(sp_peers) + n_tp - 1 + jnp.minimum(sp, 1) + jnp.minimum(n_sp - 1 - sp, 1)
    for j in range(1, n_tp):
        pl.semaphore_signal(barrier, inc=1, device_id={"tp": lax.rem(tp + j, n_tp)})

    small = [
        pltpu.make_async_copy(ld_hbm, ld_ref, in_sem.at[0]),
        pltpu.make_async_copy(fine_hbm, fine_ref, in_sem.at[1]),
        pltpu.make_async_copy(
            base_hbm.at[:, pl.ds(pl.multiple_of(sp * n_ch, n_ch), n_ch), :], base_ref, in_sem.at[2]
        ),
        pltpu.make_async_copy(gain_hbm, gain_ref, in_sem.at[3]),
    ]
    w_copies = [
        pltpu.make_async_copy(wk_hbm, wkv_ref.at[:, 0:HEAD], in_sem.at[4]),
        pltpu.make_async_copy(wv_hbm, wkv_ref.at[:, HEAD : 2 * HEAD], in_sem.at[5]),
        pltpu.make_async_copy(wp_hbm, wp_ref, in_sem.at[6]),
        pltpu.make_async_copy(wq_hbm, wqg_ref.at[:, 0:HEAD], in_sem.at[7]),
        pltpu.make_async_copy(wg_hbm, wqg_ref.at[:, HEAD : 2 * HEAD], in_sem.at[8]),
    ]

    def chunk_of(c):
        if isinstance(c, int):
            return slice(c * CHUNK, (c + 1) * CHUNK)
        return pl.ds(pl.multiple_of(c * CHUNK, CHUNK), CHUNK)

    def x_rows(c):
        return slice(HALO + c * CHUNK, HALO + (c + 1) * CHUNK)

    def tok_copy(c):
        return pltpu.make_async_copy(
            tok_hbm.at[chunk_of(c), :], x_ref.at[x_rows(c), :], tok_sem.at[c]
        )

    wout_copy = pltpu.make_async_copy(wout_hbm, wout_ref, wout_sem)

    for copy in small[:3]:
        copy.start()
    w_copies[0].start()
    w_copies[1].start()
    tok_copy(0).start()
    tok_copy(1).start()

    small[0].wait()
    w_copies[2].start()
    tok_copy(2).start()
    tok_copy(3).start()
    lc = lane_cumsum(ld_ref[...])
    lc_ref[...] = lc
    lct_ref[...] = jnp.transpose(lc)
    run = jnp.zeros((1, 1), F32)
    for c in range(n_ch):
        end = lc[2 * c : 2 * c + 1, HEAD - 1 :] + lc[2 * c + 1 : 2 * c + 2, HEAD - 1 :]
        be_ref[c : c + 1, :] = jnp.broadcast_to(jnp.exp(end), (1, HEAD))
        pre_ref[c : c + 1, :] = jnp.broadcast_to(jnp.exp(run), (1, HEAD))
        run = run + end
    tsend_ref[...] = jnp.broadcast_to(run, tsend_ref.shape)

    def columns(c):
        first = jnp.broadcast_to(lct_ref[:, 2 * c : 2 * c + 1], (HEAD, HEAD))
        second = jnp.broadcast_to(lct_ref[:, 2 * c + 1 : 2 * c + 2], (HEAD, HEAD))
        return first, second + lc_ref[2 * c : 2 * c + 1, HEAD - 1 :]

    def decay_of_chunk(c):
        row_a = lc_ref[2 * c : 2 * c + 1, :]
        row_b = lc_ref[2 * c + 1 : 2 * c + 2, :] + row_a[:, HEAD - 1 :]
        col_a, col_b = columns(c)
        low = lax.broadcasted_iota(jnp.int32, (HEAD, HEAD), 0) >= lax.broadcasted_iota(
            jnp.int32, (HEAD, HEAD), 1
        )
        sc_a, sc_b = col_a + LOG_SCALE, col_b + LOG_SCALE
        d_ref[c, :HEAD, :HEAD] = jnp.where(low, jnp.exp(sc_a - row_a), 0.0)
        d_ref[c, :HEAD, HEAD:] = jnp.zeros((HEAD, HEAD), F32)
        d_ref[c, HEAD:, :HEAD] = jnp.exp(sc_b - row_a)
        d_ref[c, HEAD:, HEAD:] = jnp.where(low, jnp.exp(sc_b - row_b), 0.0)
        here = chunk_of(c)
        within = jnp.exp(jnp.concatenate([col_a, col_b], axis=0))
        ecol_ref[here, :] = within
        edev_ref[here, :] = within * pre_ref[c : c + 1, :]

    def pushed(src, dst, slot, peer, send_sem, recv_sem, at):
        return pltpu.make_async_remote_copy(
            src_ref=src,
            dst_ref=dst.at[slot],
            send_sem=send_sem.at[at],
            recv_sem=recv_sem.at[slot],
            device_id={"sp": peer},
            device_id_type=pl.DeviceIdType.MESH,
        )

    def row_sends(j):
        return (
            pushed(tsend_ref, trecv_ref, y, row_peer(j), tsend_sem, trecv_sem, j),
            pushed(ssend_ref, srecv_ref, y, row_peer(j), ssend_sem, srecv_sem, j),
        )

    def column_sends(j):
        return (
            pushed(usend_ref, urecv_ref, z, column_peer(j), usend_sem, urecv_sem, j),
            pushed(rsend_ref, rrecv_ref, z, column_peer(j), rsend_sem, rrecv_sem, j),
        )

    small[1].wait()
    small[2].wait()
    for c in range(n_ch):
        here = chunk_of(c)
        base_c = base_ref[0, c : c + 1, :]
        base_s = base_ref[1, c : c + 1, :]
        fine_c = fine_ref[0]
        fine_s = fine_ref[1]
        cos_ref[here, :] = base_c * fine_c - base_s * fine_s
        sin_ref[here, :] = base_s * fine_c + base_c * fine_s
        col_a, col_b = columns(c)
        end = col_b[HEAD - 1 :, :] + LOG_SCALE
        fade_ref[here, :] = jnp.exp(jnp.concatenate([end - col_a, end - col_b], axis=0))
    p_ref[0 : PAD + HALO, :] = jnp.zeros((PAD + HALO, HEAD), F32)
    shift_ref[0:PAD, :] = jnp.zeros((PAD, HEAD), F32)
    for later in range(4, n_ch):
        tok_copy(later).start()
    w_copies[0].wait()
    w_copies[1].wait()
    w_copies[2].wait()

    def turned(x, c):
        here = chunk_of(c)
        return x * cos_ref[here, :] + pltpu.roll(x, HEAD // 2, 1) * sin_ref[here, :]

    x_at, core = lax.div(tp, 2), lax.rem(tp, 2)
    order = [(1, 0), (3, 0), (2, 0), (2, 1), (1, 1), (3, 1), (0, 1), (0, 0)]

    def peer_of(dx, dc):
        return lax.rem(x_at + dx, n_x) * 2 + lax.rem(core + dc, 2)

    def row_copy(peer, send_ref, recv_ref, send_sem, recv_sem):
        return pltpu.make_async_remote_copy(
            src_ref=send_ref.at[peer],
            dst_ref=recv_ref.at[tp],
            send_sem=send_sem.at[peer],
            recv_sem=recv_sem.at[tp],
            device_id={"tp": peer},
            device_id_type=pl.DeviceIdType.MESH,
        )

    def recv_wait(j, send_ref, recv_ref, send_sem, recv_sem):
        pltpu.make_async_remote_copy(
            src_ref=send_ref.at[0],
            dst_ref=recv_ref.at[j],
            send_sem=send_sem.at[0],
            recv_sem=recv_sem.at[j],
            device_id={"tp": tp},
            device_id_type=pl.DeviceIdType.MESH,
        ).wait_recv()

    group = lax.div(tp * HEAD, 256)
    window = jnp.left_shift(jnp.int32(2), group)

    def pooled_of(c):
        deep = CHUNK + HALO
        at = PAD + c * CHUNK
        x = p_ref[at : at + deep, :]
        s = x + p_ref[at - 1 : at - 1 + deep, :]
        for level in (1, 2, 3):
            shift_ref[PAD : PAD + deep, :] = s
            back = shift_ref[PAD - 2**level : PAD - 2**level + deep, :]
            s = jnp.where(group >= level, s + back, s)
        s = s[HALO:, :]
        x = x[HALO:, :]
        at = lax.broadcasted_iota(jnp.int32, (HALO, HEAD), 0) + (sp * rows + c * CHUNK + 1)
        count = jnp.minimum(at, window).astype(F32)
        whole = jnp.minimum(lax.broadcasted_iota(jnp.int32, (1, HEAD), 1) + 4096, window).astype(F32)
        top = s[:HALO, :] / count
        rest = s[HALO:, :] * (1.0 / whole)
        return (jnp.concatenate([top, rest], axis=0) - x).astype(BF16)

    p_args = (psend_ref, prow_ref, psend_sem, precv_sem)
    g_args = (gsend_ref, grow_ref, gsend_sem, grecv_sem)

    def p_of(c):
        return dot(x_ref[x_rows(c), :], wp_ref[...])

    def keep_p(c, p):
        p_ref[PAD + HALO + c * CHUNK : PAD + HALO + (c + 1) * CHUNK, :] = p
        if c > 0:
            psend_ref[c] = pooled_of(c)

    def send_pooled(*chunks):
        for c in chunks:

            @pl.when(tp != c)
            def _():
                row_copy(c, *p_args).start()

    def first_chunk():
        @pl.when(sp > 0)
        def _():
            halo_copy.wait_recv()
            p_ref[PAD : PAD + HALO, :] = halo_ref[...].astype(F32)

        psend_ref[0] = pooled_of(0)
        send_pooled(0)
        prow_ref[tp] = psend_ref[tp]

    peers = [peer_of(dx, dc) for dx, dc in order]

    def kv_of(c):
        if c == 0:
            tok_copy(0).wait()
            tok_copy(1).wait()
        if c == 2:
            tok_copy(2).wait()
            tok_copy(3).wait()
        if c == 4:
            for later in range(4, n_ch):
                tok_copy(later).wait()
            for copy in w_copies[3:]:
                copy.start()
            small[3].start()
            pl.semaphore_wait(barrier, met)
            send_pooled(*range(1, 3))
        return dot(x_ref[x_rows(c), :], wkv_ref[...])

    def keep_kv(c, kv):
        here = chunk_of(c)
        k_rot = turned(kv[:, :HEAD], c)
        k_ref[here, :] = k_rot.astype(BF16)
        v_ref[here, :] = kv[:, HEAD:].astype(BF16)
        faded_ref[c] = jnp.transpose((k_rot * fade_ref[here, :]).astype(BF16))

    def advance(c, state):
        sloc_ref[c] = state.astype(BF16)
        return state * be_ref[c : c + 1, :] + dot(faded_ref[c], v_ref[chunk_of(c), :])

    state = jnp.zeros((HEAD, HEAD), F32)
    kv = kv_of(0)
    for c in range(n_ch):
        if c + 1 < n_ch:
            kv_next = kv_of(c + 1)
        if c > 0:
            state = advance(c - 1, state)
        if c < EARLY:
            p = p_of(c)
        keep_kv(c, kv)
        if c < EARLY:
            keep_p(c, p)
        kv = kv_next
    state = advance(n_ch - 1, state)
    wout_copy.start()
    halo_send[...] = dot(x_ref[rows:, :], wp_ref[...]).astype(BF16)
    ssend_ref[...] = state.astype(BF16)
    srecv_ref[y] = state.astype(BF16)
    trecv_ref[y] = tsend_ref[...]

    halo_copy = pltpu.make_async_remote_copy(
        src_ref=halo_send,
        dst_ref=halo_ref,
        send_sem=hsend_sem,
        recv_sem=hrecv_sem,
        device_id={"sp": lax.rem(sp + 1, n_sp)},
        device_id_type=pl.DeviceIdType.MESH,
    )

    @pl.when(sp + 1 < n_sp)
    def _():
        halo_copy.start()

    for j in (3, 1, 2):
        for copy in row_sends(j):
            copy.start()

    p = p_of(EARLY)
    for c in range(EARLY, n_ch):
        if c + 1 < n_ch:
            p_next = p_of(c + 1)
        keep_p(c, p)
        for d in range(2 * (c - EARLY), min(n_ch, 2 * (c - EARLY) + 2)):
            decay_of_chunk(d)
        if c == EARLY + 1:
            send_pooled(*range(3, EARLY + 2))
        p = p_next
    send_pooled(*range(EARLY + 2, n_ch))

    w_copies[3].wait()
    w_copies[4].wait()
    def mix(c, qg):
        here = chunk_of(c)
        gate = qg[:, HEAD:]
        g_ref[here, :] = (gate * jax.nn.sigmoid(gate)).astype(BF16)
        q_rot = turned(qg[:, :HEAD], c).astype(BF16)
        q_ref[here, :] = q_rot
        return (dot_nt(q_rot, k_ref[here, :]) * d_ref[c]).astype(BF16)

    def retain(c, mixing):
        here = chunk_of(c)
        inner = dot(mixing, v_ref[here, :])
        acc_ref[here, :] = inner + dot(q_ref[here, :], sloc_ref[c]) * ecol_ref[here, :]

    def row_states():
        for j in range(1, n_y):
            slot = lax.rem(y + j, n_y)
            pushed(tsend_ref, trecv_ref, slot, sp, tsend_sem, trecv_sem, 0).wait_recv()
            pushed(ssend_ref, srecv_ref, slot, sp, ssend_sem, srecv_sem, 0).wait_recv()
        total = jnp.zeros((HEAD, HEAD), F32)
        before = jnp.zeros((HEAD, HEAD), F32)
        reach = jnp.zeros((1, HEAD), F32)
        upto = jnp.zeros((1, HEAD), F32)
        for j in range(n_y):
            before = jnp.where(y == j, total, before)
            upto = jnp.where(y == j, reach, upto)
            decay = trecv_ref[j, 0:1, :]
            total = total * jnp.exp(decay) + srecv_ref[j].astype(F32)
            reach = reach + decay
        pref_ref[...] = before
        upto_ref[...] = jnp.broadcast_to(jnp.exp(upto), upto_ref.shape)
        usend_ref[...] = jnp.broadcast_to(reach, usend_ref.shape)
        rsend_ref[...] = total.astype(BF16)
        for j in range(1, n_z):

            @pl.when(z + j < n_z)
            def _():
                for copy in column_sends(j):
                    copy.start()

    qg = dot(x_ref[x_rows(0), :], wqg_ref[...])
    mixing = None
    for c in range(n_ch):
        if c + 1 < n_ch:
            qg_next = dot(x_ref[x_rows(c + 1), :], wqg_ref[...])
        mixing_next = mix(c, qg)
        if c > 0:
            retain(c - 1, mixing)
        qg, mixing = qg_next, mixing_next
        if c == ROW_AT:

            @pl.when(y != 0)
            def _():
                row_states()

        if c == ROW_AT + 2:

            @pl.when(y == 0)
            def _():
                row_states()

        if c == HALO_AT:
            first_chunk()
    retain(n_ch - 1, mixing)

    inc_ref[...] = jnp.zeros_like(inc_ref)

    def inc_step(j, carry):
        pushed(usend_ref, urecv_ref, j, sp, usend_sem, urecv_sem, 0).wait_recv()
        pushed(rsend_ref, rrecv_ref, j, sp, rsend_sem, rrecv_sem, 0).wait_recv()
        inc_ref[...] = inc_ref[...] * jnp.exp(urecv_ref[j, 0:1, :]) + rrecv_ref[j].astype(F32)
        return carry

    lax.fori_loop(0, z, inc_step, 0)
    incoming = (inc_ref[...] * upto_ref[0:1, :] + pref_ref[...]).astype(BF16)

    small[3].wait()

    def cross_of(c):
        return dot(q_ref[chunk_of(c), :], incoming)

    def gated_of(c, cross):
        here = chunk_of(c)
        retained = acc_ref[here, :] + cross * edev_ref[here, :]
        centered = retained - jnp.mean(retained, axis=-1, keepdims=True)
        scale = lax.rsqrt(jnp.mean(centered * centered, axis=-1, keepdims=True) + 1e-06)
        return (g_ref[here, :].astype(F32) * gain_ref[...] * (centered * scale)).astype(BF16)

    cross = cross_of(peers[0])
    for k, peer in enumerate(peers):
        if k + 1 < n_tp:
            cross_next = cross_of(peers[k + 1])
        chunk = gated_of(peer, cross)
        if k + 1 < n_tp:
            gsend_ref[peer] = chunk
            row_copy(peer, *g_args).start()
        else:
            grow_ref[tp] = chunk
        cross = cross_next

    wout_copy.wait()
    for j in range(n_tp):

        @pl.when(tp != j)
        def _():
            recv_wait(j, *p_args)

    n_cols = wout_ref.shape[1]
    tile = 256
    pool_rows = jnp.concatenate([prow_ref[j] for j in range(n_tp)], axis=1)

    tiles = [slice(i * tile, (i + 1) * tile) for i in range(n_cols // tile)]
    for at in tiles:
        oacc_ref[:, at] = dot(pool_rows, wout_ref[width:, at])

    for n, dx in enumerate((0, 2, 1, 3)):
        pair = lax.rem(x_at + dx, n_x)
        if dx == 0:
            recv_wait(pair * 2 + 1 - core, *g_args)
        else:
            recv_wait(pair * 2, *g_args)
            recv_wait(pair * 2 + 1, *g_args)
        lhs = jnp.concatenate([grow_ref[pair * 2], grow_ref[pair * 2 + 1]], axis=1)
        deep = pl.ds(pl.multiple_of(pair * 2 * HEAD, 2 * HEAD), 2 * HEAD)

        for at in tiles:
            total = oacc_ref[:, at] + dot(lhs, wout_ref[deep, at])
            if n < 3:
                oacc_ref[:, at] = total
            else:
                obuf_ref[:, at] = total.astype(BF16)

    for j in range(1, n_y):
        for copy in row_sends(j):
            copy.wait_send()
    for j in range(1, n_z):

        @pl.when(z + j < n_z)
        def _():
            for copy in column_sends(j):
                copy.wait_send()

    @pl.when(sp + 1 < n_sp)
    def _():
        halo_copy.wait_send()

    for k in range(n_tp - 1):
        peer = peer_of(*order[k])
        row_copy(peer, *p_args).wait_send()
        row_copy(peer, *g_args).wait_send()


def local(n_sp, n_tp, tokens, w_query, w_key, w_value, w_gate, w_pool, norm_gain, log_decay, w_out):
    rows, depth = tokens.shape
    n_ch = rows // CHUNK
    out_rows, out_cols = rows // n_tp, w_out.shape[1]
    fine = np.stack(angle_tables(np.arange(CHUNK)))
    base = np.stack(angle_tables(np.arange(n_sp * n_ch) * CHUNK))
    any_spec = pl.BlockSpec(memory_space=pltpu.HBM)
    dma = pltpu.SemaphoreType.DMA
    vm = pltpu.VMEM
    return pl.pallas_call(
        functools.partial(kernel, n_sp, n_tp),
        out_shape=pltpu.VMEM((out_rows, out_cols), BF16),
        in_specs=[any_spec] * 11,
        out_specs=pl.BlockSpec(memory_space=pltpu.VMEM),
        scratch_shapes=[
            vm((HALO + rows, depth), BF16),
            vm((depth, 2 * HEAD), BF16),
            vm((depth, 2 * HEAD), BF16),
            vm((depth, HEAD), BF16),
            vm(w_out.shape, BF16),
            vm((1, HEAD), F32),
            vm((rows // HEAD, HEAD), F32),
            vm((2, CHUNK, HEAD), F32),
            vm((2, n_ch, HEAD), F32),
            vm((rows, HEAD), BF16),
            vm((rows, HEAD), BF16),
            vm((n_ch, HEAD, CHUNK), BF16),
            vm((rows, HEAD), BF16),
            vm((rows, HEAD), BF16),
            vm((PAD + HALO + rows, HEAD), F32),
            vm((HALO, HEAD), BF16),
            vm((HALO, HEAD), BF16),
            vm((rows, HEAD), F32),
            vm((rows // HEAD, HEAD), F32),
            vm((HEAD, rows // HEAD), F32),
            vm((rows, HEAD), F32),
            vm((rows, HEAD), F32),
            vm((rows, HEAD), F32),
            vm((PAD + HALO + CHUNK, HEAD), F32),
            vm((rows, HEAD), F32),
            vm((rows, HEAD), F32),
            vm((n_ch, CHUNK, CHUNK), F32),
            vm((n_ch, HEAD), F32),
            vm((n_ch, HEAD), F32),
            vm((n_ch, HEAD, HEAD), BF16),
            vm((HEAD, HEAD), BF16),
            vm((SIDE, HEAD, HEAD), BF16),
            vm((8, HEAD), F32),
            vm((SIDE, 8, HEAD), F32),
            vm((HEAD, HEAD), BF16),
            vm((n_sp // SIDE, HEAD, HEAD), BF16),
            vm((8, HEAD), F32),
            vm((n_sp // SIDE, 8, HEAD), F32),
            vm((HEAD, HEAD), F32),
            vm((8, HEAD), F32),
            vm((HEAD, HEAD), F32),
            vm((n_tp, CHUNK, HEAD), BF16),
            vm((n_tp, CHUNK, HEAD), BF16),
            vm((n_tp, CHUNK, HEAD), BF16),
            vm((n_tp, CHUNK, HEAD), BF16),
            vm((out_rows, out_cols), F32),
            dma((n_ch,)),
            dma((9,)),
            dma,
            dma((SIDE,)),
            dma((SIDE,)),
            dma((SIDE,)),
            dma((SIDE,)),
            dma((n_sp // SIDE,)),
            dma((n_sp // SIDE,)),
            dma((n_sp // SIDE,)),
            dma((n_sp // SIDE,)),
            dma,
            dma,
            dma((n_tp,)),
            dma((n_tp,)),
            dma((n_tp,)),
            dma((n_tp,)),
        ],
        compiler_params=pltpu.CompilerParams(
            collective_id=0, has_side_effects=True, vmem_limit_bytes=VMEM_LIMIT
        ),
        name="layer",
    )(
        tokens,
        w_query,
        w_key,
        w_value,
        w_gate,
        w_pool,
        norm_gain.reshape(1, HEAD),
        log_decay.reshape(rows // HEAD, HEAD),
        w_out,
        fine,
        base,
    )
def solution(mesh):
    in_specs = (
        P("sp", None),
        P(None, "tp"),
        P(None, "tp"),
        P(None, "tp"),
        P(None, "tp"),
        P(None, "tp"),
        P("tp"),
        P("tp", "sp"),
        P(),
    )
    body = functools.partial(local, mesh.shape["sp"], mesh.shape["tp"])
    return jax.shard_map(
        body, mesh=mesh, in_specs=in_specs, out_specs=P(("sp", "tp"), None), check_vma=False
    )
```
